512 devices in a mesh: rep: 2 (over z_hi), fs: 32 (over z_lo, y), tp: 8 (over x, core).
Axes of the slice: x: 4, y: 8, z: 8 (z_hi: 2, z_lo: 4; z = z_hi * 4 + z_lo), core: 2. Of those that a mesh axis runs over, the one named last changes fastest.
Arguments:
- tokens: bfloat16 [64, 192, 2048], P(('rep', 'fs'), 'tp'), may hold values from -6 to 6
- mix_gain: float32 [2048], replicated, may hold values from 0.1 to 1.9
- w_query: float32 [2048, 2048], P('fs', 'tp'), may hold values from -0.125 to 0.125
- w_key: float32 [2048, 2048], P('fs', 'tp'), may hold values from -0.125 to 0.125
- w_value: float32 [2048, 2048], P('fs', 'tp'), may hold values from -0.125 to 0.125
- w_out: float32 [2048, 2048], P('tp', 'fs'), may hold values from -0.125 to 0.125
- scale_query: float32 [2048], P('tp'), may hold values from 0.1 to 1.9
- scale_key: float32 [2048], P('tp'), may hold values from 0.1 to 1.9
- scale_value: float32 [2048], P('tp'), may hold values from 0.1 to 1.9
- scale_out: float32 [2048], replicated, may hold values from 0.1 to 1.9
- decay_rate: float32 [8], P('tp'), may hold values from 0.003 to 0.08
- mlp_gain: float32 [2048], replicated, may hold values from 0.1 to 1.9
- w_gate: float32 [2048, 3072], P('fs', 'tp'), may hold values from -0.125 to 0.125
- w_up: float32 [2048, 3072], P('fs', 'tp'), may hold values from -0.125 to 0.125
- w_down: float32 [3072, 2048], P('tp', 'fs'), may hold values from -0.109375 to 0.109375
- scale_gate: float32 [3072], P('tp'), may hold values from 0.1 to 1.9
- scale_up: float32 [3072], P('tp'), may hold values from 0.1 to 1.9
- scale_down: float32 [2048], replicated, may hold values from 0.1 to 1.9
Outputs:
- layer_out: bfloat16 [64, 192, 2048], P(('rep', 'fs'), 'tp')
The draws below stay inside these ranges and needn't reach their ends.
All inputs are finite; a program needn't handle non-finite values.
Results may differ from the reference program's by a relative error of at most 0.015.
Values may be sent and summed in bfloat16 or wider, within the bound.
No kernel may reach another device: no remote copies, remote signals or barrier semaphores. Data moves between devices by JAX's collectives and lax.ppermute only.
A program may use at most 64 MiB of HBM per device.

```python
import math
import jax
import jax.numpy as jnp
from jax import lax

HEADS = 8
HEAD_DIM = 256
D = 2048
FF = 3072
BLOCK = 64
SEQ_LEN = 192
SEQS = 64
N_TP = 8


def shard_levels(rng, dims, cuts, least, high):
    level, own = 1.0, jax.random.fold_in(rng, 6)
    for axis_at, blocks in cuts:
        heights = jnp.exp(jax.random.uniform(jax.random.fold_in(own, axis_at), (blocks,), jnp.float32, least / len(cuts), high / len(cuts)))
        level = level * jnp.repeat(heights, dims[axis_at] // blocks).reshape([-1 if axis == axis_at else 1 for axis in range(len(dims))])
    return level


def noise(key, shape, deviation, reach, cuts=(), kind=jnp.bfloat16):
    values = deviation * jax.random.normal(key, shape, jnp.float32)
    if cuts:
        values = values * shard_levels(key, shape, cuts, -0.22, 0.18)
    return jnp.clip(values, -reach, reach).astype(kind)


def setup_inputs(seed: int = 0) -> dict:
    seeds = jax.random.split(jax.random.key(seed), 19)
    tokens = noise(seeds[0], (SEQS, SEQ_LEN, D), 1.0, 6.0, ((0, 64), (1, 8)))
    mix_gain = jnp.clip(1.0 + 0.18 * jax.random.normal(seeds[1], (D,), jnp.float32), 0.1, 1.9)
    w_query = noise(seeds[2], (D, D), D ** -0.5, 0.125, ((0, 32), (1, 8)), jnp.float32)
    w_key = noise(seeds[3], (D, D), D ** -0.5, 0.125, ((0, 32), (1, 8)), jnp.float32)
    w_value = noise(seeds[4], (D, D), D ** -0.5, 0.125, ((0, 32), (1, 8)), jnp.float32)
    w_out = noise(seeds[5], (D, D), D ** -0.5, 0.125, ((0, 8), (1, 32)), jnp.float32)
    scale_query = jnp.clip(1.0 + 0.18 * jax.random.normal(seeds[6], (D,), jnp.float32), 0.1, 1.9)
    scale_key = jnp.clip(1.0 + 0.18 * jax.random.normal(seeds[7], (D,), jnp.float32), 0.1, 1.9)
    scale_value = jnp.clip(1.0 + 0.18 * jax.random.normal(seeds[8], (D,), jnp.float32), 0.1, 1.9)
    scale_out = jnp.clip(1.0 + 0.18 * jax.random.normal(seeds[9], (D,), jnp.float32), 0.1, 1.9)
    decay_rate = jnp.clip(jnp.exp(math.log(0.08) - 3.2834143 * jax.random.uniform(seeds[10], (HEADS,), jnp.float32) ** shard_levels(seeds[10], (HEADS,), ((0, 8),), -0.2, 0.2)), 0.003, 0.08)
    mlp_gain = jnp.clip(1.0 + 0.18 * jax.random.normal(seeds[11], (D,), jnp.float32), 0.1, 1.9)
    w_gate = noise(seeds[12], (D, FF), D ** -0.5, 0.125, ((0, 32), (1, 8)), jnp.float32)
    w_up = noise(seeds[13], (D, FF), D ** -0.5, 0.125, ((0, 32), (1, 8)), jnp.float32)
    w_down = noise(seeds[14], (FF, D), FF ** -0.5, 0.109375, ((0, 8), (1, 32)), jnp.float32)
    scale_gate = jnp.clip(1.0 + 0.18 * jax.random.normal(seeds[15], (FF,), jnp.float32), 0.1, 1.9)
    scale_up = jnp.clip(1.0 + 0.18 * jax.random.normal(seeds[16], (FF,), jnp.float32), 0.1, 1.9)
    scale_down = jnp.clip(1.0 + 0.18 * jax.random.normal(seeds[17], (D,), jnp.float32), 0.1, 1.9)
    return dict(tokens=tokens, mix_gain=mix_gain, w_query=w_query, w_key=w_key, w_value=w_value, w_out=w_out, scale_query=scale_query, scale_key=scale_key, scale_value=scale_value, scale_out=scale_out, decay_rate=decay_rate, mlp_gain=mlp_gain, w_gate=w_gate, w_up=w_up, w_down=w_down, scale_gate=scale_gate, scale_up=scale_up, scale_down=scale_down)


EPS = 1e-06
ROPE_BASE = 10000.0

def rms_scale(values, gain):
    values = values.astype(jnp.float32)
    return values * lax.rsqrt(lax.optimization_barrier(jnp.mean(values * values, axis=-1, keepdims=True)) + EPS) * gain

def rotary(values, positions):
    width = values.shape[-1]
    half = width // 2
    inv_freq = 1.0 / ROPE_BASE ** (jnp.arange(0, width, 2, dtype=jnp.float32) / width)
    angles = positions.astype(jnp.float32)[:, None] * inv_freq[None, :]
    cosine = jnp.cos(angles)[:, None, :]
    sine = jnp.sin(angles)[:, None, :]
    first = values[..., :half]
    second = values[..., half:]
    return jnp.concatenate([first * cosine - second * sine, first * sine + second * cosine], axis=-1)

def retention(query, keyed, valued, rates):
    length, heads, width = query.shape
    nblocks = length // BLOCK

    def split(values):
        return values.reshape(nblocks, BLOCK, heads, width).transpose(0, 2, 1, 3)
    log_gamma = -rates
    inside = jnp.arange(BLOCK, dtype=jnp.float32)
    distance = inside[:, None] - inside[None, :]
    inner_product = jnp.where(distance[None] >= 0.0, jnp.exp(log_gamma[:, None, None] * jnp.maximum(distance, 0.0)[None]), 0.0)
    query_decay = jnp.exp(log_gamma[:, None] * (inside[None, :] + 1.0))
    key_decay_factor = jnp.exp(log_gamma[:, None] * (BLOCK - 1.0 - inside[None, :]))
    block_decay = jnp.exp(log_gamma * BLOCK)

    def advance(state, blocks):
        query_block_tile, key_block_tile, value_block_tile = blocks
        decay_weights = (jnp.einsum('frk,fvk->frv', query_block_tile.astype(jnp.float32), key_block_tile.astype(jnp.float32)) * inner_product).astype(jnp.bfloat16)
        local = jnp.einsum('hnm,hmv->hnv', decay_weights.astype(jnp.float32), value_block_tile.astype(jnp.float32))
        carried = jnp.einsum('hnd,hdv->hnv', query_block_tile.astype(jnp.float32) * query_decay[:, :, None], state, precision=lax.Precision.HIGHEST)
        state_update = jnp.einsum('asf,asp->afp', key_block_tile.astype(jnp.float32) * key_decay_factor[:, :, None], value_block_tile.astype(jnp.float32), precision=lax.Precision.HIGHEST)
        return (state * block_decay[:, None, None] + state_update, local + carried)
    initial = jnp.zeros((heads, width, width), jnp.float32)
    _, outs = lax.scan(advance, initial, (split(query), split(keyed), split(valued)))
    return outs.transpose(0, 2, 1, 3).reshape(length, heads, width)

def group_sum(inputs, weight, scale):
    length, inner_width = inputs.shape
    pieces = inputs.reshape(length, N_TP, inner_width // N_TP).astype(jnp.float32)
    blocks = weight.reshape(N_TP, inner_width // N_TP, weight.shape[1]).astype(jnp.float32)
    terms = jnp.einsum('ltc,tcd->ltd', pieces, blocks) * scale
    return lax.optimization_barrier(jnp.sum(terms.astype(jnp.bfloat16).astype(jnp.float32), axis=1))

def reference(tokens, mix_gain, w_query, w_key, w_value, w_out, scale_query, scale_key, scale_value, scale_out, decay_rate, mlp_gain, w_gate, w_up, w_down, scale_gate, scale_up, scale_down):
    query_w = w_query.astype(jnp.bfloat16)
    key_w = w_key.astype(jnp.bfloat16)
    value_w = w_value.astype(jnp.bfloat16)
    out_w = w_out.astype(jnp.bfloat16)
    gate_w = w_gate.astype(jnp.bfloat16)
    up_w = w_up.astype(jnp.bfloat16)
    down_w = w_down.astype(jnp.bfloat16)

    def one_sequence(rows):
        length = rows.shape[0]
        positions = jnp.arange(length)
        normed = rms_scale(rows, mix_gain).astype(jnp.bfloat16)
        query_raw = jnp.dot(normed, query_w, preferred_element_type=jnp.float32) * scale_query
        key_raw = jnp.dot(normed, key_w, preferred_element_type=jnp.float32) * scale_key
        value_raw = jnp.dot(normed, value_w, preferred_element_type=jnp.float32) * scale_value
        query_rows = rotary(query_raw.reshape(length, HEADS, HEAD_DIM), positions).astype(jnp.bfloat16)
        key_rows = rotary(key_raw.reshape(length, HEADS, HEAD_DIM), positions).astype(jnp.bfloat16)
        value_rows = value_raw.reshape(length, HEADS, HEAD_DIM).astype(jnp.bfloat16)
        retained = retention(query_rows, key_rows, value_rows, decay_rate)
        attended = rms_scale(retained, 1.0).astype(jnp.bfloat16).reshape(length, D)
        mixed = group_sum(attended, out_w, scale_out)
        hidden_state = (rows.astype(jnp.float32) + mixed).astype(jnp.bfloat16)
        mlp_in = rms_scale(hidden_state, mlp_gain).astype(jnp.bfloat16)
        gate_val = jnp.dot(mlp_in, gate_w, preferred_element_type=jnp.float32) * scale_gate
        up_val = jnp.dot(mlp_in, up_w, preferred_element_type=jnp.float32) * scale_up
        inner_product = (jax.nn.silu(gate_val) * up_val).astype(jnp.bfloat16)
        channel = group_sum(inner_product, down_w, scale_down)
        return (hidden_state.astype(jnp.float32) + channel).astype(jnp.bfloat16)
    return lax.map(one_sequence, tokens)
```

```python
import jax
import jax.numpy as jnp
from jax import lax
from jax.sharding import Mesh, PartitionSpec as P

HEAD_DIM = 256
EPS = 1e-06
ROPE_BASE = 10000.0
RING = ("rep", "z")
TP = ("x", "core")


def inv_rms(values):
    return lax.rsqrt(jnp.mean(values * values, axis=-1, keepdims=True) + EPS)


def broadcast_exchange(array, axis):
    peers = lax.axis_size(axis)
    return lax.all_to_all(
        jnp.broadcast_to(array[None], (peers, *array.shape)), axis, 0, 0, tiled=True
    )


def pairs(offset, n=8):
    out = []
    for a in range(offset, n + offset, 2):
        b = (a + 1) % n
        out += [(a % n, b), (b, a % n)]
    return out


def ring_pieces(block):
    half = block.shape[0] // 2
    even = lax.ppermute(block, RING, pairs(0))
    odd = lax.ppermute(block, RING, pairs(1))
    far_a = lax.ppermute(even[:half], RING, pairs(1))
    far_b = lax.ppermute(odd[half:], RING, pairs(0))
    return block, even, odd, far_a, far_b


def ring_labels():
    z = lax.axis_index("z")
    odd = z % 2
    even_label = z + 1 - 2 * odd
    odd_label = (z + 3 + 2 * odd) % 4
    return z, even_label, odd_label, (z + 2) % 4


def ring_dot(x, pieces, dot):
    own, even, odd, far_a, far_b = pieces
    size = own.shape[0]
    half = size // 2
    lo, le, lod, lf = ring_labels()

    def cut(label, start, length):
        return lax.dynamic_slice_in_dim(x, label * size + start, length, 1)

    total = dot(cut(lo, 0, size), own)
    total = total + dot(cut(le, 0, size), even)
    total = total + dot(cut(lod, 0, size), odd)
    total = total + dot(cut(lf, 0, half), far_a)
    return total + dot(cut(lf, half, half), far_b)


def dot(a, b):
    return jnp.dot(a, b, preferred_element_type=jnp.float32)


def dot_t(a, b):
    return lax.dot_general(a, b, (((1,), (1,)), ((), ())), preferred_element_type=jnp.float32)


def rotary(values, cosine, sine):
    half = values.shape[-1] // 2
    first = values[:, :half]
    second = values[:, half:]
    return jnp.concatenate(
        [first * cosine - second * sine, first * sine + second * cosine], axis=-1
    )


def per_device(
    tokens,
    mix_gain,
    w_query,
    w_key,
    w_value,
    w_out,
    scale_query,
    scale_key,
    scale_value,
    scale_out,
    decay_rate,
    mlp_gain,
    w_gate,
    w_up,
    w_down,
    scale_gate,
    scale_up,
    scale_down,
):
    bf16, f32 = jnp.bfloat16, jnp.float32
    own_rows = tokens[0]
    rows, width = own_rows.shape
    length = rows * lax.axis_size(TP)
    rep = lax.axis_index("rep")
    hidden_units = w_gate.shape[1]
    half = hidden_units // 2

    qkv = jnp.concatenate([w_query, w_key, w_value], axis=1).astype(bf16)
    qkv_y = broadcast_exchange(qkv, "y").reshape(-1, qkv.shape[1])

    def my_half(w):
        return jnp.where(rep == 0, w[:, :half], w[:, half:])

    mlp_own = jnp.concatenate(
        [my_half(w_gate), my_half(w_up), my_half(w_down.T)], axis=1
    ).astype(bf16)
    mlp_all = lax.all_gather(mlp_own, ("rep", "z", "y"), axis=0, tiled=True).reshape(
        2, width, 3 * half
    )
    out_whole = broadcast_exchange(w_out.T.astype(bf16), ("z", "y")).reshape(width, -1)
    all_rows = broadcast_exchange(own_rows, TP).reshape(length, width)
    pieces = ring_pieces(qkv_y)

    values = all_rows.astype(f32)
    normed = (values * inv_rms(values) * mix_gain).astype(bf16)
    product = ring_dot(normed, pieces, dot)
    positions = jnp.arange(length, dtype=f32)
    inv_freq = 1.0 / ROPE_BASE ** (jnp.arange(0, HEAD_DIM, 2, dtype=f32) / HEAD_DIM)
    angles = positions[:, None] * inv_freq[None, :]
    cosine, sine = jnp.cos(angles), jnp.sin(angles)
    query = rotary(product[:, :HEAD_DIM] * scale_query, cosine, sine).astype(bf16)
    keyed = rotary(product[:, HEAD_DIM : 2 * HEAD_DIM] * scale_key, cosine, sine).astype(bf16)
    valued = (product[:, 2 * HEAD_DIM :] * scale_value).astype(bf16)
    distance = positions[:, None] - positions[None, :]
    decay = jnp.where(distance >= 0.0, jnp.exp(-decay_rate[0] * jnp.maximum(distance, 0.0)), 0.0)
    weights = (dot_t(query, keyed) * decay).astype(bf16)
    retained = dot(weights, valued)
    attended = (retained * inv_rms(retained)).astype(bf16)
    partial = dot_t(attended, out_whole).astype(bf16)

    terms = lax.all_to_all(partial.reshape(-1, rows, width), TP, 0, 0, tiled=True)
    mixed = jnp.sum(terms.astype(f32), axis=0) * scale_out
    hidden = (own_rows.astype(f32) + mixed).astype(bf16)
    values = hidden.astype(f32)
    mlp_in = (values * inv_rms(values) * mlp_gain).astype(bf16)
    mlp_in = lax.all_gather(mlp_in, TP, axis=0, tiled=True)

    partial = 0.0
    for r in range(2):
        both = dot(mlp_in, mlp_all[r, :, : 2 * half])
        at = slice(r * half, (r + 1) * half)
        gate = both[:, :half] * scale_gate[at]
        up = both[:, half:] * scale_up[at]
        inner = (jax.nn.silu(gate) * up).astype(bf16)
        partial = partial + dot_t(inner, mlp_all[r, :, 2 * half :])
    terms = lax.all_to_all(
        partial.astype(bf16).reshape(-1, rows, width), TP, 0, 0, tiled=True
    )
    channel = jnp.sum(terms.astype(f32), axis=0) * scale_down
    return (hidden.astype(f32) + channel).astype(bf16)[None]


def solution(mesh):
    grid = Mesh(mesh.devices.reshape(2, 4, 8, 4, 2), ("rep", "z", "y", "x", "core"))
    seqs, fs = ("rep", "z", "y"), ("z", "y")
    by_rows, by_cols = P(fs, TP), P(TP, fs)
    in_specs = (
        P(seqs, TP, None), P(), by_rows, by_rows, by_rows, by_cols,
        P(TP), P(TP), P(TP), P(), P(TP), P(),
        by_rows, by_rows, by_cols, P(TP), P(TP), P(),
    )
    return jax.shard_map(
        per_device, mesh=grid, in_specs=in_specs, out_specs=P(seqs, TP, None), check_vma=False
    )
```

```python
import jax
import jax.numpy as jnp
from jax import lax
from jax.sharding import Mesh, PartitionSpec as P


HEAD_DIM = 256
EPS = 1e-06
ROPE_BASE = 10000.0
RING = ("rep", "z")
TP = ("x", "core")


def inv_rms(values):
    return lax.rsqrt(jnp.mean(values * values, axis=-1, keepdims=True) + EPS)


def exchange_y(array):
    peers = lax.axis_size("y")
    return lax.all_to_all(
        jnp.broadcast_to(array[None], (peers, *array.shape)), "y", 0, 0, tiled=True
    )


def pairs(offset, n=8):
    out = []
    for a in range(offset, n + offset, 2):
        b = (a + 1) % n
        out += [(a % n, b), (b, a % n)]
    return out


def ring_pieces(block):
    half = block.shape[0] // 2
    even = lax.ppermute(block, RING, pairs(0))
    odd = lax.ppermute(block, RING, pairs(1))
    far_a = lax.ppermute(even[:half], RING, pairs(1))
    far_b = lax.ppermute(odd[half:], RING, pairs(0))
    return block, even, odd, far_a, far_b


def ring_labels():
    z = lax.axis_index("z")
    odd = z % 2
    return z, z + 1 - 2 * odd, (z + 3 + 2 * odd) % 4, (z + 2) % 4


def ring_slots():
    z, even, odd, _ = ring_labels()
    return [jnp.where(z == j, 0, jnp.where(even == j, 1, jnp.where(odd == j, 2, 3))) for j in range(4)]


def ring_dot(x, pieces):
    own, even, odd, far_a, far_b = pieces
    size = own.shape[0]
    half = size // 2
    own_at, even_at, odd_at, far_at = ring_labels()

    def term(label, start, piece):
        cut = lax.dynamic_slice_in_dim(x, label * size + start, piece.shape[0], 1)
        return jnp.dot(cut, piece, preferred_element_type=jnp.float32)

    total = term(own_at, 0, own) + term(even_at, 0, even) + term(odd_at, 0, odd)
    return total + term(far_at, 0, far_a) + term(far_at, half, far_b)


def dot_t(a, b):
    return lax.dot_general(a, b, (((1,), (1,)), ((), ())), preferred_element_type=jnp.float32)


def sum_at_owner(partial):
    chips = lax.axis_size("x")
    core, chip = lax.axis_index("core"), lax.axis_index("x")
    blocks = partial.reshape(chips, 2, -1, partial.shape[1])
    sent = lax.dynamic_index_in_dim(blocks, 1 - core, 1, keepdims=False)
    got = lax.ppermute(sent, "core", [(0, 1), (1, 0)])
    kept = lax.dynamic_index_in_dim(blocks, core, 1, keepdims=False)
    both = kept.astype(jnp.float32) + got.astype(jnp.float32)
    total = lax.dynamic_index_in_dim(both, chip, 0, keepdims=False)
    both = both.astype(jnp.bfloat16)
    for step in (1, 3, 2):
        block = lax.dynamic_index_in_dim(both, (chip + step) % chips, 0, keepdims=False)
        got = lax.ppermute(block, "x", [(i, (i + step) % chips) for i in range(chips)])
        total = total + got.astype(jnp.float32)
    return total


def rotary(values, cosine, sine):
    half = values.shape[-1] // 2
    first = values[:, :half]
    second = values[:, half:]
    return jnp.concatenate(
        [first * cosine - second * sine, first * sine + second * cosine], axis=-1
    )


def per_device(
    tokens,
    mix_gain,
    w_query,
    w_key,
    w_value,
    w_out,
    scale_query,
    scale_key,
    scale_value,
    scale_out,
    decay_rate,
    mlp_gain,
    w_gate,
    w_up,
    w_down,
    scale_gate,
    scale_up,
    scale_down,
):
    bf16, f32 = jnp.bfloat16, jnp.float32
    own_rows = tokens[0]
    rows, width = own_rows.shape
    length = rows * lax.axis_size(TP)
    cols = HEAD_DIM + HEAD_DIM // 2

    qkv = jnp.concatenate([w_query, w_key, w_value], axis=1).astype(bf16)
    first = exchange_y(qkv[:, :cols]).reshape(-1, cols)
    second = exchange_y(jnp.concatenate([qkv[:, cols:], w_out.T.astype(bf16)], axis=1))
    second = second.reshape(-1, cols + HEAD_DIM)
    first = ring_pieces(first)
    out_own = second[:, cols:]
    second = ring_pieces(second[:, :cols])
    out_pieces = ring_pieces(out_own)
    units = w_gate.shape[1]
    mlp = jnp.concatenate([w_gate, w_up], axis=1).astype(bf16)
    mlp = exchange_y(mlp).reshape(-1, mlp.shape[1])
    mlp = ring_pieces(mlp)
    own, even, odd, far_a, far_b = ring_pieces(w_down.T.astype(bf16))
    down = jnp.stack([own, even, odd, jnp.concatenate([far_a, far_b], axis=0)])
    down = exchange_y(down)
    down = jnp.moveaxis(down, 0, 1).reshape(width, -1)
    all_rows = lax.all_gather(own_rows, TP, axis=0, tiled=True)

    values = all_rows.astype(f32)
    normed = (values * inv_rms(values) * mix_gain).astype(bf16)
    first = ring_dot(normed, first)
    second = ring_dot(normed, second)
    positions = jnp.arange(length, dtype=f32)
    inv_freq = 1.0 / ROPE_BASE ** (jnp.arange(0, HEAD_DIM, 2, dtype=f32) / HEAD_DIM)
    angles = positions[:, None] * inv_freq[None, :]
    cosine, sine = jnp.cos(angles), jnp.sin(angles)
    key_raw = jnp.concatenate([first[:, HEAD_DIM:], second[:, : HEAD_DIM // 2]], axis=1)
    query = rotary(first[:, :HEAD_DIM] * scale_query, cosine, sine).astype(bf16)
    keyed = rotary(key_raw * scale_key, cosine, sine).astype(bf16)
    valued = (second[:, HEAD_DIM // 2 :] * scale_value).astype(bf16)
    distance = positions[:, None] - positions[None, :]
    decay = jnp.where(distance >= 0.0, jnp.exp(-decay_rate[0] * jnp.maximum(distance, 0.0)), 0.0)
    weights = (dot_t(query, keyed) * decay).astype(bf16)
    retained = jnp.dot(weights, valued, preferred_element_type=f32)
    attended = (retained * inv_rms(retained)).astype(bf16)
    partial = jnp.concatenate([dot_t(attended, piece) for piece in out_pieces], axis=1).astype(bf16)

    slots = ring_slots()

    def in_order(values):
        size = width // 4
        return jnp.concatenate(
            [lax.dynamic_slice_in_dim(values, slot * size, size, 1) for slot in slots], axis=1
        )

    mixed = sum_at_owner(partial)
    mixed = in_order(mixed) * scale_out
    hidden = (own_rows.astype(f32) + mixed).astype(bf16)
    values = hidden.astype(f32)
    mlp_in = (values * inv_rms(values) * mlp_gain).astype(bf16)
    mlp_in = lax.all_gather(mlp_in, TP, axis=0, tiled=True)

    both = ring_dot(mlp_in, mlp)
    inner = (jax.nn.silu(both[:, :units] * scale_gate) * (both[:, units:] * scale_up)).astype(bf16)
    channel = sum_at_owner(dot_t(inner, down).astype(bf16))
    channel = in_order(channel) * scale_down
    return (hidden.astype(f32) + channel).astype(bf16)[None]


def solution(mesh):
    grid = Mesh(mesh.devices.reshape(2, 4, 8, 4, 2), ("rep", "z", "y", "x", "core"))
    seqs, fs = ("rep", "z", "y"), ("z", "y")
    by_rows, by_cols = P(fs, TP), P(TP, fs)
    in_specs = (
        P(seqs, TP, None), P(), by_rows, by_rows, by_rows, by_cols,
        P(TP), P(TP), P(TP), P(), P(TP), P(),
        by_rows, by_rows, by_cols, P(TP), P(TP), P(),
    )

    return jax.shard_map(
        per_device, mesh=grid, in_specs=in_specs, out_specs=P(seqs, TP, None), check_vma=False
    )
```

```python
import jax
import jax.numpy as jnp
from jax import lax
from jax.experimental import pallas as pl
from jax.experimental.pallas import tpu as pltpu
from jax.sharding import Mesh, PartitionSpec as P


HEAD_DIM = 256
EPS = 1e-06
ROPE_BASE = 10000.0
RING = ("rep", "z")
TP = ("x", "core")


def inv_rms(values):
    return lax.rsqrt(jnp.mean(values * values, axis=-1, keepdims=True) + EPS)


def exchange_y(array):
    peers = lax.axis_size("y")
    return lax.all_to_all(
        jnp.broadcast_to(array[None], (peers, *array.shape)), "y", 0, 0, tiled=True
    )


def pairs(offset, n=8):
    out = []
    for a in range(offset, n + offset, 2):
        b = (a + 1) % n
        out += [(a % n, b), (b, a % n)]
    return out


def ring_pieces(block):
    half = block.shape[0] // 2
    even = lax.ppermute(block, RING, pairs(0))
    odd = lax.ppermute(block, RING, pairs(1))
    far_a = lax.ppermute(even[:half], RING, pairs(1))
    far_b = lax.ppermute(odd[half:], RING, pairs(0))
    return block, even, odd, far_a, far_b


def ring_labels():
    z = lax.axis_index("z")
    odd = z % 2
    return z, z + 1 - 2 * odd, (z + 3 + 2 * odd) % 4, (z + 2) % 4


def ring_slots():
    z, even, odd, _ = ring_labels()
    return [jnp.where(z == j, 0, jnp.where(even == j, 1, jnp.where(odd == j, 2, 3))) for j in range(4)]


def ring_dot(x, pieces):
    own, even, odd, far_a, far_b = pieces
    size = own.shape[0]
    half = size // 2
    own_at, even_at, odd_at, far_at = ring_labels()

    def term(label, start, piece):
        cut = lax.dynamic_slice_in_dim(x, label * size + start, piece.shape[0], 1)
        return jnp.dot(cut, piece, preferred_element_type=jnp.float32)

    total = term(own_at, 0, own) + term(even_at, 0, even) + term(odd_at, 0, odd)
    return total + term(far_at, 0, far_a) + term(far_at, half, far_b)


def dot_t(a, b):
    return lax.dot_general(a, b, (((1,), (1,)), ((), ())), preferred_element_type=jnp.float32)


def sum_at_owner(partial):
    blocks = partial.reshape(lax.axis_size(TP), -1, partial.shape[1])
    return jnp.sum(lax.all_to_all(blocks, TP, 0, 0, tiled=True).astype(jnp.float32), axis=0)


def mlp_kernel(labels, x, weights, scale_gate, scale_up, out, held, sems):
    units = scale_gate.shape[1]
    copies = [
        pltpu.make_async_copy(weights.at[:, p], held.at[p], sems.at[p]) for p in range(4)
    ]
    for copy in copies:
        copy.start()
    size = x.shape[1] // 4
    both = jnp.zeros((x.shape[0], 2 * units), jnp.float32)
    places = [pl.ds(pl.multiple_of(labels[p] * size, size), size) for p in range(4)]
    for p in range(4):
        copies[p].wait()
        piece = held[p, :, :, : 2 * units].reshape(size, 2 * units)
        both += jnp.dot(x[:, places[p]], piece, preferred_element_type=jnp.float32)
    gate = both[:, :units] * scale_gate[...]
    up = both[:, units:] * scale_up[...]
    inner = (gate / (1.0 + jnp.exp(-gate)) * up).astype(jnp.bfloat16)
    for p in range(4):
        piece = held[p, :, :, 2 * units :].reshape(size, units)
        out[:, places[p]] = dot_t(inner, piece).astype(jnp.bfloat16)


def mlp(labels, x, weights, scale_gate, scale_up):
    vmem = pl.BlockSpec(memory_space=pltpu.VMEM)
    flops = 2 * x.shape[0] * x.shape[1] * weights.shape[-1]
    return pl.pallas_call(
        mlp_kernel,
        out_shape=jax.ShapeDtypeStruct(x.shape, jnp.bfloat16),
        in_specs=[
            pl.BlockSpec(memory_space=pltpu.SMEM),
            vmem,
            pl.BlockSpec(memory_space=pl.ANY),
            vmem,
            vmem,
        ],
        out_specs=vmem,
        scratch_shapes=[
            pltpu.VMEM((4, weights.shape[0], *weights.shape[2:]), jnp.bfloat16),
            pltpu.SemaphoreType.DMA((4,)),
        ],
        compiler_params=pltpu.CompilerParams(vmem_limit_bytes=20 * 2**20),
        cost_estimate=pl.CostEstimate(
            flops=flops, bytes_accessed=2 * weights.size, transcendentals=0
        ),
        name="mlp",
    )(labels, x, weights, scale_gate[None], scale_up[None])


def rotary(values, cosine, sine):
    half = values.shape[-1] // 2
    first = values[:, :half]
    second = values[:, half:]
    return jnp.concatenate(
        [first * cosine - second * sine, first * sine + second * cosine], axis=-1
    )


def per_device(
    tokens,
    mix_gain,
    w_query,
    w_key,
    w_value,
    w_out,
    scale_query,
    scale_key,
    scale_value,
    scale_out,
    decay_rate,
    mlp_gain,
    w_gate,
    w_up,
    w_down,
    scale_gate,
    scale_up,
    scale_down,
):
    bf16, f32 = jnp.bfloat16, jnp.float32
    own_rows = tokens[0]
    rows, width = own_rows.shape
    length = rows * lax.axis_size(TP)
    heads = 3 * HEAD_DIM

    own = jnp.concatenate([w_query, w_key, w_value, w_out.T], axis=1).astype(bf16)
    both = exchange_y(own).reshape(-1, own.shape[1])
    own = jnp.concatenate([w_gate, w_up, w_down.T], axis=1).astype(bf16)
    own, even, odd, far_a, far_b = ring_pieces(own)
    own = jnp.concatenate([own, even, odd, far_a, far_b], axis=0)
    own = own.reshape(4, -1, own.shape[1])
    mlp_weights = lax.all_gather(own, "y", axis=0)
    qkv = ring_pieces(both[:, :heads])
    out_pieces = ring_pieces(both[:, heads:])
    all_rows = lax.all_gather(own_rows, TP, axis=0, tiled=True)

    values = all_rows.astype(f32)
    normed = (values * inv_rms(values) * mix_gain).astype(bf16)
    product = ring_dot(normed, qkv)
    positions = jnp.arange(length, dtype=f32)
    inv_freq = 1.0 / ROPE_BASE ** (jnp.arange(0, HEAD_DIM, 2, dtype=f32) / HEAD_DIM)
    angles = positions[:, None] * inv_freq[None, :]
    cosine, sine = jnp.cos(angles), jnp.sin(angles)
    query = rotary(product[:, :HEAD_DIM] * scale_query, cosine, sine).astype(bf16)
    keyed = rotary(product[:, HEAD_DIM : 2 * HEAD_DIM] * scale_key, cosine, sine).astype(bf16)
    valued = (product[:, 2 * HEAD_DIM :] * scale_value).astype(bf16)
    distance = positions[:, None] - positions[None, :]
    decay = jnp.where(distance >= 0.0, jnp.exp(-decay_rate[0] * jnp.maximum(distance, 0.0)), 0.0)
    weights = (dot_t(query, keyed) * decay).astype(bf16)
    retained = jnp.dot(weights, valued, preferred_element_type=f32)
    attended = (retained * inv_rms(retained)).astype(bf16)
    partial = jnp.concatenate([dot_t(attended, piece) for piece in out_pieces], axis=1).astype(bf16)

    slots = ring_slots()

    def in_order(values):
        size = width // 4
        return jnp.concatenate(
            [lax.dynamic_slice_in_dim(values, slot * size, size, 1) for slot in slots], axis=1
        )

    mixed = sum_at_owner(partial)
    mixed = in_order(mixed) * scale_out
    hidden = (own_rows.astype(f32) + mixed).astype(bf16)
    values = hidden.astype(f32)
    mlp_in = (values * inv_rms(values) * mlp_gain).astype(bf16)
    mlp_in = lax.all_gather(mlp_in, TP, axis=0, tiled=True)

    labels = jnp.stack(ring_labels()).astype(jnp.int32)
    channel = sum_at_owner(mlp(labels, mlp_in, mlp_weights, scale_gate, scale_up)) * scale_down
    return (hidden.astype(f32) + channel).astype(bf16)[None]


def solution(mesh):
    grid = Mesh(mesh.devices.reshape(2, 4, 8, 4, 2), ("rep", "z", "y", "x", "core"))
    seqs, fs = ("rep", "z", "y"), ("z", "y")
    by_rows, by_cols = P(fs, TP), P(TP, fs)
    in_specs = (
        P(seqs, TP, None), P(), by_rows, by_rows, by_rows, by_cols,
        P(TP), P(TP), P(TP), P(), P(TP), P(),
        by_rows, by_rows, by_cols, P(TP), P(TP), P(),
    )

    return jax.shard_map(
        per_device, mesh=grid, in_specs=in_specs, out_specs=P(seqs, TP, None), check_vma=False
    )
```

```python
import jax
import jax.numpy as jnp
from jax import lax
from jax.experimental import pallas as pl
from jax.experimental.pallas import tpu as pltpu
from jax.sharding import Mesh, PartitionSpec as P


HEAD_DIM = 256
EPS = 1e-06
ROPE_BASE = 10000.0
RING = ("rep", "z")
TP = ("x", "core")
CHUNKS = 4


def inv_rms(values):
    return lax.rsqrt(jnp.mean(values * values, axis=-1, keepdims=True) + EPS)


def exchange_y(array):
    peers = lax.axis_size("y")
    return lax.all_to_all(
        jnp.broadcast_to(array[None], (peers, *array.shape)), "y", 0, 0, tiled=True
    )


def pairs(offset, n=8):
    out = []
    for a in range(offset, n + offset, 2):
        b = (a + 1) % n
        out += [(a % n, b), (b, a % n)]
    return out


def ring_pieces(block):
    half = block.shape[0] // 2
    even = lax.ppermute(block, RING, pairs(0))
    odd = lax.ppermute(block, RING, pairs(1))
    far_a = lax.ppermute(even[:half], RING, pairs(1))
    far_b = lax.ppermute(odd[half:], RING, pairs(0))
    return block, even, odd, far_a, far_b


def ring_labels():
    z = lax.axis_index("z")
    odd = z % 2
    return z, z + 1 - 2 * odd, (z + 3 + 2 * odd) % 4, (z + 2) % 4


def ring_slots():
    z, even, odd, _ = ring_labels()
    return [jnp.where(z == j, 0, jnp.where(even == j, 1, jnp.where(odd == j, 2, 3))) for j in range(4)]


def ring_dot(x, pieces):
    own, even, odd, far_a, far_b = pieces
    size = own.shape[0]
    half = size // 2
    own_at, even_at, odd_at, far_at = ring_labels()

    def term(label, start, piece):
        cut = lax.dynamic_slice_in_dim(x, label * size + start, piece.shape[0], 1)
        return jnp.dot(cut, piece, preferred_element_type=jnp.float32)

    total = term(own_at, 0, own) + term(even_at, 0, even) + term(odd_at, 0, odd)
    return total + term(far_at, 0, far_a) + term(far_at, half, far_b)


def dot_t(a, b):
    return lax.dot_general(a, b, (((1,), (1,)), ((), ())), preferred_element_type=jnp.float32)


def sum_at_owner(partial):
    blocks = partial.reshape(lax.axis_size(TP), -1, partial.shape[1])
    return jnp.sum(lax.all_to_all(blocks, TP, 0, 0, tiled=True).astype(jnp.float32), axis=0)


def mlp_kernel(x, weights, scale_gate, scale_up, out, held, sems):
    units = scale_gate.shape[1]
    size = x.shape[1] // CHUNKS
    places = [pl.ds(p * size, size) for p in range(CHUNKS)]

    def fetch(r, p):
        at = (r, places[p])
        return pltpu.make_async_copy(weights.at[at], held.at[at], sems.at[r, p])

    copies = [[fetch(r, p) for p in range(CHUNKS)] for r in range(2)]
    for r in range(2):
        for copy in copies[r]:
            copy.start()
    inner = []
    for r in range(2):
        both = jnp.zeros((x.shape[0], 2 * units), jnp.float32)
        for copy, at in zip(copies[r], places):
            copy.wait()
            both += jnp.dot(
                x[:, at], held[r, at, : 2 * units], preferred_element_type=jnp.float32
            )
        gate = both[:, :units] * scale_gate[r : r + 1]
        up = both[:, units:] * scale_up[r : r + 1]
        inner.append((gate / (1.0 + jnp.exp(-gate)) * up).astype(jnp.bfloat16))
    for at in places:
        total = dot_t(inner[0], held[0, at, 2 * units :]) + dot_t(inner[1], held[1, at, 2 * units :])
        out[:, at] = total.astype(jnp.bfloat16)


def mlp(x, weights, scale_gate, scale_up):
    vmem = pl.BlockSpec(memory_space=pltpu.VMEM)
    flops = 2 * x.shape[0] * weights.size
    return pl.pallas_call(
        mlp_kernel,
        out_shape=jax.ShapeDtypeStruct(x.shape, jnp.bfloat16),
        in_specs=[vmem, pl.BlockSpec(memory_space=pltpu.HBM), vmem, vmem],
        out_specs=vmem,
        scratch_shapes=[
            pltpu.VMEM(weights.shape, jnp.bfloat16),
            pltpu.SemaphoreType.DMA((2, CHUNKS)),
        ],
        compiler_params=pltpu.CompilerParams(vmem_limit_bytes=60 * 2**20),
        cost_estimate=pl.CostEstimate(
            flops=flops, bytes_accessed=2 * weights.size, transcendentals=0
        ),
        name="mlp",
    )(x, weights, scale_gate.reshape(2, -1), scale_up.reshape(2, -1))


def rotary(values, cosine, sine):
    half = values.shape[-1] // 2
    first = values[:, :half]
    second = values[:, half:]
    return jnp.concatenate(
        [first * cosine - second * sine, first * sine + second * cosine], axis=-1
    )


def per_device(
    tokens,
    mix_gain,
    w_query,
    w_key,
    w_value,
    w_out,
    scale_query,
    scale_key,
    scale_value,
    scale_out,
    decay_rate,
    mlp_gain,
    w_gate,
    w_up,
    w_down,
    scale_gate,
    scale_up,
    scale_down,
):
    bf16, f32 = jnp.bfloat16, jnp.float32
    own_rows = tokens[0]
    rows, width = own_rows.shape
    length = rows * lax.axis_size(TP)
    heads = 3 * HEAD_DIM

    own = jnp.concatenate([w_query, w_key, w_value, w_out.T], axis=1).astype(bf16)
    both = exchange_y(own).reshape(-1, own.shape[1])
    half = w_gate.shape[1] // 2
    low = lax.axis_index("rep") == 0
    own = [
        jnp.where(low, w[:, :half], w[:, half:]) for w in (w_gate, w_up, w_down.T)
    ]
    own = jnp.concatenate(own, axis=1).astype(bf16)
    mlp_weights = lax.all_gather(own, ("rep", "z", "y"), axis=0, tiled=True)
    mlp_weights = mlp_weights.reshape(2, width, -1)
    qkv = ring_pieces(both[:, :heads])
    out_pieces = ring_pieces(both[:, heads:])
    all_rows = lax.all_gather(own_rows, TP, axis=0, tiled=True)

    values = all_rows.astype(f32)
    normed = (values * inv_rms(values) * mix_gain).astype(bf16)
    product = ring_dot(normed, qkv)
    positions = jnp.arange(length, dtype=f32)
    inv_freq = 1.0 / ROPE_BASE ** (jnp.arange(0, HEAD_DIM, 2, dtype=f32) / HEAD_DIM)
    angles = positions[:, None] * inv_freq[None, :]
    cosine, sine = jnp.cos(angles), jnp.sin(angles)
    query = rotary(product[:, :HEAD_DIM] * scale_query, cosine, sine).astype(bf16)
    keyed = rotary(product[:, HEAD_DIM : 2 * HEAD_DIM] * scale_key, cosine, sine).astype(bf16)
    valued = (product[:, 2 * HEAD_DIM :] * scale_value).astype(bf16)
    distance = positions[:, None] - positions[None, :]
    decay = jnp.where(distance >= 0.0, jnp.exp(-decay_rate[0] * jnp.maximum(distance, 0.0)), 0.0)
    weights = (dot_t(query, keyed) * decay).astype(bf16)
    retained = jnp.dot(weights, valued, preferred_element_type=f32)
    attended = (retained * inv_rms(retained)).astype(bf16)
    partial = jnp.concatenate([dot_t(attended, piece) for piece in out_pieces], axis=1).astype(bf16)

    slots = ring_slots()

    def in_order(values):
        size = width // 4
        return jnp.concatenate(
            [lax.dynamic_slice_in_dim(values, slot * size, size, 1) for slot in slots], axis=1
        )

    mixed = sum_at_owner(partial)
    mixed = in_order(mixed) * scale_out
    hidden = (own_rows.astype(f32) + mixed).astype(bf16)
    values = hidden.astype(f32)
    mlp_in = (values * inv_rms(values) * mlp_gain).astype(bf16)
    mlp_in = lax.all_gather(mlp_in, TP, axis=0, tiled=True)

    channel = sum_at_owner(mlp(mlp_in, mlp_weights, scale_gate, scale_up)) * scale_down
    return (hidden.astype(f32) + channel).astype(bf16)[None]


def solution(mesh):
    grid = Mesh(mesh.devices.reshape(2, 4, 8, 4, 2), ("rep", "z", "y", "x", "core"))
    seqs, fs = ("rep", "z", "y"), ("z", "y")
    by_rows, by_cols = P(fs, TP), P(TP, fs)
    in_specs = (
        P(seqs, TP, None), P(), by_rows, by_rows, by_rows, by_cols,
        P(TP), P(TP), P(TP), P(), P(TP), P(),
        by_rows, by_rows, by_cols, P(TP), P(TP), P(),
    )

    return jax.shard_map(
        per_device, mesh=grid, in_specs=in_specs, out_specs=P(seqs, TP, None), check_vma=False
    )
```

```python
import jax
import jax.numpy as jnp
from jax import lax
from jax.experimental import pallas as pl
from jax.experimental.pallas import tpu as pltpu
from jax.sharding import Mesh, PartitionSpec as P


HEAD_DIM = 256
EPS = 1e-06
ROPE_BASE = 10000.0
RING = ("rep", "z")
TP = ("x", "core")


def inv_rms(values):
    return lax.rsqrt(jnp.mean(values * values, axis=-1, keepdims=True) + EPS)


def pairs(offset, n=8):
    out = []
    for a in range(offset, n + offset, 2):
        b = (a + 1) % n
        out += [(a % n, b), (b, a % n)]
    return out


def ring_pieces(block):
    half = block.shape[0] // 2
    even = lax.ppermute(block, RING, pairs(0))
    odd = lax.ppermute(block, RING, pairs(1))
    far_a = lax.ppermute(even[:half], RING, pairs(1))
    far_b = lax.ppermute(odd[half:], RING, pairs(0))
    return block, even, odd, far_a, far_b


def ring_labels():
    z = lax.axis_index("z")
    odd = z % 2
    return z, z + 1 - 2 * odd, (z + 3 + 2 * odd) % 4, (z + 2) % 4


def ring_slots():
    z, even, odd, _ = ring_labels()
    return [jnp.where(z == j, 0, jnp.where(even == j, 1, jnp.where(odd == j, 2, 3))) for j in range(4)]


def ring_blocks(block):
    even = lax.ppermute(block, RING, pairs(0))
    odd = lax.ppermute(block, RING, pairs(1))
    far = lax.ppermute(block, RING, [(i, (i + 2) % 8) for i in range(8)])
    return jnp.stack([block, even, odd, far])


def ring_dot(x, pieces, columns):
    size = pieces[0].shape[0]
    half = size // 2
    own_at, even_at, odd_at, far_at = ring_labels()
    starts = (own_at * size, even_at * size, odd_at * size, far_at * size, far_at * size + half)

    def term(start, piece):
        cut = lax.dynamic_slice_in_dim(x, start, piece.shape[0], 1)
        return jnp.dot(cut, piece[:, :columns], preferred_element_type=jnp.float32)

    return sum(term(start, piece) for start, piece in zip(starts, pieces))


def dot_t(a, b):
    return lax.dot_general(a, b, (((1,), (1,)), ((), ())), preferred_element_type=jnp.float32)


def sum_at_owner(partial):
    blocks = partial.reshape(lax.axis_size(TP), -1, partial.shape[1])
    return jnp.sum(lax.all_to_all(blocks, TP, 0, 0, tiled=True).astype(jnp.float32), axis=0)


def rotary(values, cosine, sine):
    half = values.shape[-1] // 2
    first = values[:, :half]
    second = values[:, half:]
    return jnp.concatenate(
        [first * cosine - second * sine, first * sine + second * cosine], axis=-1
    )


VMEM = pl.BlockSpec(memory_space=pltpu.VMEM)
SMEM = pl.BlockSpec(memory_space=pltpu.SMEM)


def local_call(kernel, out_shape, specs, flops=0, moved=0):
    return pl.pallas_call(
        kernel,
        out_shape=out_shape,
        in_specs=specs,
        out_specs=VMEM,
        compiler_params=pltpu.CompilerParams(vmem_limit_bytes=24 * 2**20),
        cost_estimate=pl.CostEstimate(flops=flops, bytes_accessed=moved, transcendentals=0),
    )


def heads_shard_kernel(query, keyed, valued, out_w, out):
    width = query.shape[1]
    parts = [ref[...].astype(jnp.bfloat16) for ref in (query, keyed, valued, out_w)]
    for peer in range(out.shape[0]):
        for i, part in enumerate(parts):
            out[peer, :, i * width : (i + 1) * width] = part


def heads_shard(w_query, w_key, w_value, w_out, peers):
    rows, width = w_query.shape
    shape = jax.ShapeDtypeStruct((peers, rows, 4 * width), jnp.bfloat16)
    return local_call(heads_shard_kernel, shape, [VMEM] * 4, 10**7, 2**21)(
        w_query, w_key, w_value, w_out.T
    )


def mlp_shard_kernel(gate, up, down, out):
    units = gate.shape[1]
    out[:, :units] = gate[...].astype(jnp.bfloat16)
    out[:, units : 2 * units] = up[...].astype(jnp.bfloat16)
    out[:, 2 * units :] = down[...].astype(jnp.bfloat16)


def mlp_shard(w_gate, w_up, w_down):
    rows, units = w_gate.shape
    shape = jax.ShapeDtypeStruct((rows, 3 * units), jnp.bfloat16)
    return local_call(mlp_shard_kernel, shape, [VMEM] * 3, 10**7, 2**20)(w_gate, w_up, w_down.T)


def retain_kernel(rate, product, cosine, sine, sq, sk, sv, own, even, odd, far_a, far_b, out):
    width = sq.shape[1]
    cos, sin = cosine[...], sine[...]
    query = rotary(product[:, :width] * sq[...], cos, sin).astype(jnp.bfloat16)
    keyed = rotary(product[:, width : 2 * width] * sk[...], cos, sin).astype(jnp.bfloat16)
    valued = (product[:, 2 * width :] * sv[...]).astype(jnp.bfloat16)
    length = product.shape[0]
    after = lax.broadcasted_iota(jnp.int32, (length, length), 0)
    before = lax.broadcasted_iota(jnp.int32, (length, length), 1)
    distance = (after - before).astype(jnp.float32)
    decay = jnp.exp(-rate[0] * jnp.maximum(distance, 0.0))
    weights = jnp.where(distance >= 0.0, dot_t(query, keyed) * decay, 0.0).astype(jnp.bfloat16)
    retained = jnp.dot(weights, valued, preferred_element_type=jnp.float32)
    attended = (retained * inv_rms(retained)).astype(jnp.bfloat16)
    at = 0
    for piece in (own, even, odd, far_a, far_b):
        to = at + piece.shape[0]
        out[:, at:to] = dot_t(attended, piece[:, 3 * width :]).astype(jnp.bfloat16)
        at = to


def retain(rate, product, cosine, sine, scales, pieces):
    columns = sum(piece.shape[0] for piece in pieces)
    shape = jax.ShapeDtypeStruct((product.shape[0], columns), jnp.bfloat16)
    specs = [SMEM] + [VMEM] * (6 + len(pieces))
    scales = [scale[None] for scale in scales]
    return local_call(retain_kernel, shape, specs, 3 * 10**8, 2**21)(
        rate, product, cosine, sine, *scales, *pieces
    )


def mlp_kernel(labels, x, weights, scale_gate, scale_up, out):
    units = scale_gate.shape[1]
    size = x.shape[1] // 4
    both = jnp.zeros((x.shape[0], 2 * units), jnp.float32)
    places = [pl.ds(pl.multiple_of(labels[p] * size, size), size) for p in range(4)]
    for p, at in enumerate(places):
        piece = weights[:, p, :, : 2 * units].reshape(size, 2 * units)
        both += jnp.dot(x[:, at], piece, preferred_element_type=jnp.float32)
    gate = both[:, :units] * scale_gate[...]
    up = both[:, units:] * scale_up[...]
    inner = (gate / (1.0 + jnp.exp(-gate)) * up).astype(jnp.bfloat16)
    for p, at in enumerate(places):
        piece = weights[:, p, :, 2 * units :].reshape(size, units)
        out[:, at] = dot_t(inner, piece).astype(jnp.bfloat16)


def mlp(labels, x, weights, scale_gate, scale_up):
    shape = jax.ShapeDtypeStruct(x.shape, jnp.bfloat16)
    flops = 2 * x.shape[0] * x.shape[1] * weights.shape[-1]
    return local_call(mlp_kernel, shape, [SMEM] + [VMEM] * 4, flops, 2 * weights.size)(
        labels, x, weights, scale_gate[None], scale_up[None]
    )


def per_device(
    tokens,
    mix_gain,
    w_query,
    w_key,
    w_value,
    w_out,
    scale_query,
    scale_key,
    scale_value,
    scale_out,
    decay_rate,
    mlp_gain,
    w_gate,
    w_up,
    w_down,
    scale_gate,
    scale_up,
    scale_down,
):
    bf16, f32 = jnp.bfloat16, jnp.float32
    own_rows = tokens[0]
    rows, width = own_rows.shape
    length = rows * lax.axis_size(TP)
    peers = lax.axis_size("y")
    heads = heads_shard(w_query, w_key, w_value, w_out, peers)
    heads = lax.all_to_all(heads, "y", 0, 0, tiled=True).reshape(-1, heads.shape[2])
    own = ring_blocks(mlp_shard(w_gate, w_up, w_down))
    mlp_weights = lax.all_gather(own, "y", axis=0)
    heads = ring_pieces(heads)
    all_rows = lax.all_gather(own_rows, TP, axis=0, tiled=True)

    values = all_rows.astype(f32)
    normed = (values * inv_rms(values) * mix_gain).astype(bf16)
    product = ring_dot(normed, heads, 3 * HEAD_DIM)
    positions = jnp.arange(length, dtype=f32)
    inv_freq = 1.0 / ROPE_BASE ** (jnp.arange(0, HEAD_DIM, 2, dtype=f32) / HEAD_DIM)
    angles = positions[:, None] * inv_freq[None, :]
    scales = (scale_query, scale_key, scale_value)
    partial = retain(decay_rate, product, jnp.cos(angles), jnp.sin(angles), scales, heads)

    slots = ring_slots()

    def in_order(values):
        size = width // 4
        return jnp.concatenate(
            [lax.dynamic_slice_in_dim(values, slot * size, size, 1) for slot in slots], axis=1
        )

    mixed = sum_at_owner(partial)
    mixed = in_order(mixed) * scale_out
    hidden = (own_rows.astype(f32) + mixed).astype(bf16)
    values = hidden.astype(f32)
    mlp_in = (values * inv_rms(values) * mlp_gain).astype(bf16)
    mlp_in = lax.all_gather(mlp_in, TP, axis=0, tiled=True)

    labels = jnp.stack(ring_labels()).astype(jnp.int32)
    channel = sum_at_owner(mlp(labels, mlp_in, mlp_weights, scale_gate, scale_up)) * scale_down
    return (hidden.astype(f32) + channel).astype(bf16)[None]


def solution(mesh):
    grid = Mesh(mesh.devices.reshape(2, 4, 8, 4, 2), ("rep", "z", "y", "x", "core"))
    seqs, fs = ("rep", "z", "y"), ("z", "y")
    by_rows, by_cols = P(fs, TP), P(TP, fs)
    in_specs = (
        P(seqs, TP, None), P(), by_rows, by_rows, by_rows, by_cols,
        P(TP), P(TP), P(TP), P(), P(TP), P(),
        by_rows, by_rows, by_cols, P(TP), P(TP), P(),
    )

    return jax.shard_map(
        per_device, mesh=grid, in_specs=in_specs, out_specs=P(seqs, TP, None), check_vma=False
    )
```

```python
import jax
import jax.numpy as jnp
from jax import lax
from jax.experimental import pallas as pl
from jax.experimental.pallas import tpu as pltpu
from jax.sharding import Mesh, PartitionSpec as P


HEAD_DIM = 256
EPS = 1e-06
ROPE_BASE = 10000.0
RING = ("rep", "z")
TP = ("x", "core")


def inv_rms(values):
    return lax.rsqrt(jnp.mean(values * values, axis=-1, keepdims=True) + EPS)


def pairs(offset, n=8):
    out = []
    for a in range(offset, n + offset, 2):
        b = (a + 1) % n
        out += [(a % n, b), (b, a % n)]
    return out


def ring_pieces(block):
    half = block.shape[0] // 2
    even = lax.ppermute(block, RING, pairs(0))
    odd = lax.ppermute(block, RING, pairs(1))
    far_a = lax.ppermute(even[:half], RING, pairs(1))
    far_b = lax.ppermute(odd[half:], RING, pairs(0))
    return block, even, odd, far_a, far_b


def ring_labels():
    z = lax.axis_index("z")
    odd = z % 2
    return z, z + 1 - 2 * odd, (z + 3 + 2 * odd) % 4, (z + 2) % 4


def ring_slots():
    z, even, odd, _ = ring_labels()
    return [jnp.where(z == j, 0, jnp.where(even == j, 1, jnp.where(odd == j, 2, 3))) for j in range(4)]


def ring_blocks(block):
    even = lax.ppermute(block, RING, pairs(0))
    odd = lax.ppermute(block, RING, pairs(1))
    far = lax.ppermute(block, RING, [(i, (i + 2) % 8) for i in range(8)])
    return jnp.stack([block, even, odd, far])


def ring_dot(x, pieces, columns):
    size = pieces[0].shape[0]
    half = size // 2
    own_at, even_at, odd_at, far_at = ring_labels()
    starts = (own_at * size, even_at * size, odd_at * size, far_at * size, far_at * size + half)

    def term(start, piece):
        cut = lax.dynamic_slice_in_dim(x, start, piece.shape[0], 1)
        return jnp.dot(cut, piece[:, :columns], preferred_element_type=jnp.float32)

    return sum(term(start, piece) for start, piece in zip(starts, pieces))


def dot_t(a, b):
    return lax.dot_general(a, b, (((1,), (1,)), ((), ())), preferred_element_type=jnp.float32)


def sum_over_chips(partial):
    blocks = partial.reshape(lax.axis_size("x"), -1, partial.shape[1])
    return jnp.sum(lax.all_to_all(blocks, "x", 0, 0, tiled=True).astype(jnp.float32), axis=0)


def swap_cores(array):
    return lax.ppermute(array, "core", [(0, 1), (1, 0)])


def rotary(values, cosine, sine):
    half = values.shape[-1] // 2
    first = values[:, :half]
    second = values[:, half:]
    return jnp.concatenate(
        [first * cosine - second * sine, first * sine + second * cosine], axis=-1
    )


VMEM = pl.BlockSpec(memory_space=pltpu.VMEM)
SMEM = pl.BlockSpec(memory_space=pltpu.SMEM)


def local_call(kernel, out_shape, specs, flops, moved, out_specs=VMEM):
    return pl.pallas_call(
        kernel,
        out_shape=out_shape,
        in_specs=specs,
        out_specs=out_specs,
        compiler_params=pltpu.CompilerParams(vmem_limit_bytes=24 * 2**20),
        cost_estimate=pl.CostEstimate(flops=flops, bytes_accessed=moved, transcendentals=0),
    )


def heads_shard_kernel(query, keyed, valued, out_w, out, held, sems):
    width = query.shape[1]
    parts = (query, keyed, valued, out_w)
    copies = [pltpu.make_async_copy(w, held.at[i], sems.at[i]) for i, w in enumerate(parts)]
    for copy in copies:
        copy.start()
    for i, copy in enumerate(copies):
        copy.wait()
        part = held[i].astype(jnp.bfloat16)
        for peer in range(out.shape[0]):
            out[peer, :, i * width : (i + 1) * width] = part


def heads_shard(w_query, w_key, w_value, w_out, peers):
    rows, width = w_query.shape
    return pl.pallas_call(
        heads_shard_kernel,
        out_shape=jax.ShapeDtypeStruct((peers, rows, 4 * width), jnp.bfloat16),
        in_specs=[pl.BlockSpec(memory_space=pltpu.HBM)] * 4,
        out_specs=VMEM,
        scratch_shapes=[
            pltpu.VMEM((4, rows, width), jnp.float32),
            pltpu.SemaphoreType.DMA((4,)),
        ],
        compiler_params=pltpu.CompilerParams(vmem_limit_bytes=60 * 2**20),
        cost_estimate=pl.CostEstimate(flops=10**7, bytes_accessed=2**21, transcendentals=0),
        name="heads_shard",
    )(w_query, w_key, w_value, w_out.T)


def mlp_shard_kernel(gate, up, down, out):
    units = gate.shape[1]
    out[:, :units] = gate[...].astype(jnp.bfloat16)
    out[:, units : 2 * units] = up[...].astype(jnp.bfloat16)
    out[:, 2 * units :] = down[...].astype(jnp.bfloat16)


def mlp_shard(w_gate, w_up, w_down):
    rows, units = w_gate.shape
    shape = jax.ShapeDtypeStruct((rows, 3 * units), jnp.bfloat16)
    return local_call(mlp_shard_kernel, shape, [VMEM] * 3, 10**7, 2**20)(w_gate, w_up, w_down.T)


def retain_kernel(rate, core, product, cosine, sine, sq, sk, sv, own, even, odd, far_a, far_b, kept, sent):
    width = sq.shape[1]
    cos, sin = cosine[...], sine[...]
    query = rotary(product[:, :width] * sq[...], cos, sin).astype(jnp.bfloat16)
    keyed = rotary(product[:, width : 2 * width] * sk[...], cos, sin).astype(jnp.bfloat16)
    valued = (product[:, 2 * width :] * sv[...]).astype(jnp.bfloat16)
    length = product.shape[0]
    after = lax.broadcasted_iota(jnp.int32, (length, length), 0)
    before = lax.broadcasted_iota(jnp.int32, (length, length), 1)
    distance = (after - before).astype(jnp.float32)
    decay = jnp.exp(-rate[0] * jnp.maximum(distance, 0.0))
    weights = jnp.where(distance >= 0.0, dot_t(query, keyed) * decay, 0.0).astype(jnp.bfloat16)
    retained = jnp.dot(weights, valued, preferred_element_type=jnp.float32)
    attended = retained * inv_rms(retained)
    rows = length // 8
    first = [attended[i * rows : (i + 1) * rows] for i in range(0, 8, 2)]
    second = [attended[i * rows : (i + 1) * rows] for i in range(1, 8, 2)]
    low = core[0] == 0
    mine = [jnp.where(low, a, b) for a, b in zip(first, second)]
    other = [jnp.where(low, b, a) for a, b in zip(first, second)]
    attended = jnp.concatenate(mine + other, axis=0).astype(jnp.bfloat16)
    half = length // 2
    at = 0
    for piece in (own, even, odd, far_a, far_b):
        to = at + piece.shape[0]
        term = dot_t(attended, piece[:, 3 * width :])
        kept[:, at:to] = term[:half]
        sent[:, at:to] = term[half:].astype(jnp.bfloat16)
        at = to


def retain(rate, core, product, cosine, sine, scales, pieces):
    columns = sum(piece.shape[0] for piece in pieces)
    half = product.shape[0] // 2
    shapes = [jax.ShapeDtypeStruct((half, columns), kind) for kind in (jnp.float32, jnp.bfloat16)]
    specs = [SMEM] * 2 + [VMEM] * (6 + len(pieces))
    scales = [scale[None] for scale in scales]
    return local_call(retain_kernel, shapes, specs, 3 * 10**8, 2**21, [VMEM] * 2)(
        rate, core, product, cosine, sine, *scales, *pieces
    )


def hold_kernel(weights, out):
    out[...] = weights[...]


def hold(weights):
    shape = jax.ShapeDtypeStruct(weights.shape, weights.dtype)
    return local_call(hold_kernel, shape, [VMEM], 10**7, 4 * weights.size)(weights)


def mlp_kernel(labels, x, weights, others, scales, other_scales, out):
    units = scales.shape[1]
    size = x.shape[1] // 4
    places = [pl.ds(pl.multiple_of(labels[p] * size, size), size) for p in range(4)]
    inner = []
    for held, scale in ((weights, scales), (others, other_scales)):
        both = jnp.zeros((x.shape[0], 2 * units), jnp.float32)
        for p, at in enumerate(places):
            piece = held[:, p, :, : 2 * units].reshape(size, 2 * units)
            both += jnp.dot(x[:, at], piece, preferred_element_type=jnp.float32)
        gate = both[:, :units] * scale[0:1]
        up = both[:, units:] * scale[1:2]
        inner.append((gate / (1.0 + jnp.exp(-gate)) * up).astype(jnp.bfloat16))
    for p, at in enumerate(places):
        total = 0.0
        for held, part in zip((weights, others), inner):
            total += dot_t(part, held[:, p, :, 2 * units :].reshape(size, units))
        out[:, at] = total.astype(jnp.bfloat16)


def mlp(labels, x, weights, others, scales, other_scales):
    shape = jax.ShapeDtypeStruct(x.shape, jnp.bfloat16)
    flops = 4 * x.shape[0] * x.shape[1] * weights.shape[-1]
    return local_call(mlp_kernel, shape, [SMEM] + [VMEM] * 5, flops, 4 * weights.size)(
        labels, x, weights, others, scales, other_scales
    )


def per_device(
    tokens,
    mix_gain,
    w_query,
    w_key,
    w_value,
    w_out,
    scale_query,
    scale_key,
    scale_value,
    scale_out,
    decay_rate,
    mlp_gain,
    w_gate,
    w_up,
    w_down,
    scale_gate,
    scale_up,
    scale_down,
):
    bf16, f32 = jnp.bfloat16, jnp.float32
    own_rows = tokens[0]
    rows, width = own_rows.shape
    length = rows * lax.axis_size(TP)
    peers = lax.axis_size("y")
    heads = heads_shard(w_query, w_key, w_value, w_out, peers)
    heads = lax.all_to_all(heads, "y", 0, 0, tiled=True).reshape(-1, heads.shape[2])
    own = ring_blocks(mlp_shard(w_gate, w_up, w_down))
    mlp_weights = lax.all_gather(own, "y", axis=0)
    mlp_weights = hold(mlp_weights)
    mlp_others = swap_cores(mlp_weights)
    mlp_scales = jnp.stack([scale_gate, scale_up])
    other_scales = swap_cores(mlp_scales)
    heads = ring_pieces(heads)
    all_rows = lax.all_gather(own_rows, TP, axis=0, tiled=True)

    values = all_rows.astype(f32)
    normed = (values * inv_rms(values) * mix_gain).astype(bf16)
    product = ring_dot(normed, heads, 3 * HEAD_DIM)
    positions = jnp.arange(length, dtype=f32)
    inv_freq = 1.0 / ROPE_BASE ** (jnp.arange(0, HEAD_DIM, 2, dtype=f32) / HEAD_DIM)
    angles = positions[:, None] * inv_freq[None, :]
    scales = (scale_query, scale_key, scale_value)
    core = lax.axis_index("core").astype(jnp.int32)[None]
    kept, sent = retain(
        decay_rate, core, product, jnp.cos(angles), jnp.sin(angles), scales, heads
    )

    slots = ring_slots()

    def in_order(values):
        size = width // 4
        return jnp.concatenate(
            [lax.dynamic_slice_in_dim(values, slot * size, size, 1) for slot in slots], axis=1
        )

    got = swap_cores(sent)
    mixed = sum_over_chips((kept + got.astype(f32)).astype(bf16))
    mixed = in_order(mixed) * scale_out
    hidden = (own_rows.astype(f32) + mixed).astype(bf16)
    values = hidden.astype(f32)
    mlp_in = (values * inv_rms(values) * mlp_gain).astype(bf16)
    copies = jnp.broadcast_to(mlp_in[None], (lax.axis_size("x"), rows, width))
    mlp_in = lax.all_to_all(copies, "x", 0, 0, tiled=True).reshape(-1, width)

    labels = jnp.stack(ring_labels()).astype(jnp.int32)
    partial = mlp(labels, mlp_in, mlp_weights, mlp_others, mlp_scales, other_scales)
    channel = sum_over_chips(partial) * scale_down
    return (hidden.astype(f32) + channel).astype(bf16)[None]


def solution(mesh):
    grid = Mesh(mesh.devices.reshape(2, 4, 8, 4, 2), ("rep", "z", "y", "x", "core"))
    seqs, fs = ("rep", "z", "y"), ("z", "y")
    by_rows, by_cols = P(fs, TP), P(TP, fs)
    in_specs = (
        P(seqs, TP, None), P(), by_rows, by_rows, by_rows, by_cols,
        P(TP), P(TP), P(TP), P(), P(TP), P(),
        by_rows, by_rows, by_cols, P(TP), P(TP), P(),
    )

    return jax.shard_map(
        per_device, mesh=grid, in_specs=in_specs, out_specs=P(seqs, TP, None), check_vma=False
    )
```

```python
import jax
import jax.numpy as jnp
from jax import lax
from jax.experimental import pallas as pl
from jax.experimental.pallas import tpu as pltpu
from jax.sharding import Mesh, PartitionSpec as P


HEAD_DIM = 256
EPS = 1e-06
ROPE_BASE = 10000.0
RING = ("rep", "z")
TP = ("x", "core")


def inv_rms(values):
    return lax.rsqrt(jnp.mean(values * values, axis=-1, keepdims=True) + EPS)


def pairs(offset, n=8):
    out = []
    for a in range(offset, n + offset, 2):
        b = (a + 1) % n
        out += [(a % n, b), (b, a % n)]
    return out


def ring_pieces(block):
    half = block.shape[0] // 2
    even = lax.ppermute(block, RING, pairs(0))
    odd = lax.ppermute(block, RING, pairs(1))
    far_a = lax.ppermute(even[:half], RING, pairs(1))
    far_b = lax.ppermute(odd[half:], RING, pairs(0))
    return block, even, odd, far_a, far_b


def ring_halves(block):
    half = block.shape[0] // 2
    low, high = block[:half], block[half:]
    even1 = lax.ppermute(low, RING, pairs(0))
    odd2 = lax.ppermute(high, RING, pairs(1))
    even2 = lax.ppermute(high, RING, pairs(0))
    odd1 = lax.ppermute(low, RING, pairs(1))
    far_a = lax.ppermute(even1, RING, pairs(1))
    far_b = lax.ppermute(odd2, RING, pairs(0))
    return block, even1, even2, odd1, odd2, far_a, far_b


def ring_labels():
    z = lax.axis_index("z")
    odd = z % 2
    return z, z + 1 - 2 * odd, (z + 3 + 2 * odd) % 4, (z + 2) % 4


def ring_slots():
    z, even, odd, _ = ring_labels()
    return [jnp.where(z == j, 0, jnp.where(even == j, 1, jnp.where(odd == j, 2, 3))) for j in range(4)]


def ring_blocks(block):
    even = lax.ppermute(block, RING, pairs(0))
    odd = lax.ppermute(block, RING, pairs(1))
    far = lax.ppermute(block, RING, [(i, (i + 2) % 8) for i in range(8)])
    return jnp.stack([block, even, odd, far])


def ring_dot(x, pieces, columns):
    size = pieces[0].shape[0]
    half = size // 2
    own_at, even_at, odd_at, far_at = [label * size for label in ring_labels()]
    starts = (own_at, even_at, even_at + half, odd_at, odd_at + half, far_at, far_at + half)

    def term(start, piece):
        cut = lax.dynamic_slice_in_dim(x, start, piece.shape[0], 1)
        return jnp.dot(cut, piece[:, :columns], preferred_element_type=jnp.float32)

    return sum(term(start, piece) for start, piece in zip(starts, pieces))


def dot_t(a, b):
    return lax.dot_general(a, b, (((1,), (1,)), ((), ())), preferred_element_type=jnp.float32)


def swap_cores(array):
    return lax.ppermute(array, "core", [(0, 1), (1, 0)])


def rotary(values, cosine, sine):
    half = values.shape[-1] // 2
    first = values[:, :half]
    second = values[:, half:]
    return jnp.concatenate(
        [first * cosine - second * sine, first * sine + second * cosine], axis=-1
    )


VMEM = pl.BlockSpec(memory_space=pltpu.VMEM)
SMEM = pl.BlockSpec(memory_space=pltpu.SMEM)


def local_call(kernel, out_shape, specs, flops, moved, out_specs=VMEM):
    return pl.pallas_call(
        kernel,
        out_shape=out_shape,
        in_specs=specs,
        out_specs=out_specs,
        compiler_params=pltpu.CompilerParams(vmem_limit_bytes=24 * 2**20),
        cost_estimate=pl.CostEstimate(flops=flops, bytes_accessed=moved, transcendentals=0),
    )


def heads_shard_kernel(query, keyed, valued, out_w, out, held, sems):
    width = query.shape[1]
    parts = (query, keyed, valued, out_w)
    copies = [pltpu.make_async_copy(w, held.at[i], sems.at[i]) for i, w in enumerate(parts)]
    for copy in copies:
        copy.start()
    for i, copy in enumerate(copies):
        copy.wait()
        part = held[i].astype(jnp.bfloat16)
        for peer in range(out.shape[0]):
            out[peer, :, i * width : (i + 1) * width] = part


def heads_shard(w_query, w_key, w_value, w_out, peers):
    rows, width = w_query.shape
    return pl.pallas_call(
        heads_shard_kernel,
        out_shape=jax.ShapeDtypeStruct((peers, rows, 4 * width), jnp.bfloat16),
        in_specs=[pl.BlockSpec(memory_space=pltpu.HBM)] * 4,
        out_specs=VMEM,
        scratch_shapes=[
            pltpu.VMEM((4, rows, width), jnp.float32),
            pltpu.SemaphoreType.DMA((4,)),
        ],
        compiler_params=pltpu.CompilerParams(vmem_limit_bytes=60 * 2**20),
        cost_estimate=pl.CostEstimate(flops=10**7, bytes_accessed=2**21, transcendentals=0),
        name="heads_shard",
    )(w_query, w_key, w_value, w_out.T)


def mlp_shard_kernel(gate, up, down, both, downs):
    units = gate.shape[1]
    both[:, :units] = gate[...].astype(jnp.bfloat16)
    both[:, units:] = up[...].astype(jnp.bfloat16)
    part = down[...].astype(jnp.bfloat16)
    for peer in range(downs.shape[0]):
        downs[peer] = part


def mlp_shard(w_gate, w_up, w_down, peers):
    rows, units = w_gate.shape
    shapes = [(rows, 2 * units), (peers, rows, units)]
    shapes = [jax.ShapeDtypeStruct(shape, jnp.bfloat16) for shape in shapes]
    call = local_call(mlp_shard_kernel, shapes, [VMEM] * 3, 10**7, 2**20, [VMEM] * 2)
    return call(w_gate, w_up, w_down.T)


def retain_kernel(rate, core, product, cosine, sine, sq, sk, sv, *refs):
    pieces, (kept, sent) = refs[:-2], refs[-2:]
    width = sq.shape[1]
    cos, sin = cosine[...], sine[...]
    query = rotary(product[:, :width] * sq[...], cos, sin).astype(jnp.bfloat16)
    keyed = rotary(product[:, width : 2 * width] * sk[...], cos, sin).astype(jnp.bfloat16)
    valued = (product[:, 2 * width :] * sv[...]).astype(jnp.bfloat16)
    length = product.shape[0]
    after = lax.broadcasted_iota(jnp.int32, (length, length), 0)
    before = lax.broadcasted_iota(jnp.int32, (length, length), 1)
    distance = (after - before).astype(jnp.float32)
    decay = jnp.exp(-rate[0] * jnp.maximum(distance, 0.0))
    weights = jnp.where(distance >= 0.0, dot_t(query, keyed) * decay, 0.0).astype(jnp.bfloat16)
    retained = jnp.dot(weights, valued, preferred_element_type=jnp.float32)
    attended = retained * inv_rms(retained)
    rows = length // 8
    first = [attended[i * rows : (i + 1) * rows] for i in range(0, 8, 2)]
    second = [attended[i * rows : (i + 1) * rows] for i in range(1, 8, 2)]
    low = core[0] == 0
    mine = [jnp.where(low, a, b) for a, b in zip(first, second)]
    other = [jnp.where(low, b, a) for a, b in zip(first, second)]
    attended = jnp.concatenate(mine + other, axis=0).astype(jnp.bfloat16)
    half = length // 2
    at = 0
    for piece in pieces:
        to = at + piece.shape[0]
        term = dot_t(attended, piece[:, 3 * width :])
        kept[:, at:to] = term[:half]
        sent[:, at:to] = term[half:].astype(jnp.bfloat16)
        at = to


def retain(rate, core, product, cosine, sine, scales, pieces):
    columns = sum(piece.shape[0] for piece in pieces)
    half = product.shape[0] // 2
    shapes = [jax.ShapeDtypeStruct((half, columns), kind) for kind in (jnp.float32, jnp.bfloat16)]
    specs = [SMEM] * 2 + [VMEM] * (6 + len(pieces))
    scales = [scale[None] for scale in scales]
    return local_call(retain_kernel, shapes, specs, 3 * 10**8, 2**21, [VMEM] * 2)(
        rate, core, product, cosine, sine, *scales, *pieces
    )


def hold_kernel(weights, out, sem):
    copy = pltpu.make_async_copy(weights, out, sem)
    copy.start()
    copy.wait()


def hold(weights):
    return pl.pallas_call(
        hold_kernel,
        out_shape=jax.ShapeDtypeStruct(weights.shape, weights.dtype),
        in_specs=[pl.BlockSpec(memory_space=pltpu.HBM)],
        out_specs=VMEM,
        scratch_shapes=[pltpu.SemaphoreType.DMA],
        compiler_params=pltpu.CompilerParams(vmem_limit_bytes=16 * 2**20),
        cost_estimate=pl.CostEstimate(flops=10**7, bytes_accessed=2**22, transcendentals=0),
        name="hold",
    )(weights)


def settle_kernel(slots, terms, own, scale, gain, hidden, copies):
    size = own.shape[1] // 4
    total = 0.0
    for j in range(4):
        at = slice(j * size, (j + 1) * size)
        there = pl.ds(pl.multiple_of(slots[j] * size, size), size)
        mixed = jnp.sum(terms[:, :, there].astype(jnp.float32), axis=0) * scale[:, at]
        block = (own[:, at].astype(jnp.float32) + mixed).astype(jnp.bfloat16)
        hidden[:, at] = block
        block = block.astype(jnp.float32)
        total += jnp.sum(block * block, axis=-1, keepdims=True)
    factor = lax.rsqrt(total / own.shape[1] + EPS)
    for j in range(4):
        at = slice(j * size, (j + 1) * size)
        block = (hidden[:, at].astype(jnp.float32) * factor * gain[:, at]).astype(jnp.bfloat16)
        for peer in range(copies.shape[0]):
            copies[peer, :, at] = block


def settle(slots, terms, own, scale, gain):
    shapes = [jax.ShapeDtypeStruct(a.shape, jnp.bfloat16) for a in (own, terms)]
    call = local_call(settle_kernel, shapes, [SMEM] + [VMEM] * 4, 10**7, 2**19, [VMEM] * 2)
    return call(slots, terms, own, scale[None], gain[None])


def pack_kernel(*refs):
    at = 0
    for piece in refs[:-1]:
        refs[-1][at : at + piece.shape[0]] = piece[...]
        at += piece.shape[0]


def pack(pieces):
    rows = sum(piece.shape[0] for piece in pieces)
    shape = jax.ShapeDtypeStruct((rows, pieces[0].shape[1]), jnp.bfloat16)
    return local_call(pack_kernel, shape, [VMEM] * len(pieces), 10**7, 2**22)(*pieces)


def mlp_kernel(labels, x, weights, others, down, other_down, scales, other_scales, out):
    units = scales.shape[1]
    size = x.shape[1] // 4
    places = [pl.ds(pl.multiple_of(labels[p] * size, size), size) for p in range(4)]
    inner = []
    for held, scale in ((weights, scales), (others, other_scales)):
        both = jnp.zeros((x.shape[0], 2 * units), jnp.float32)
        for p, at in enumerate(places):
            piece = held[:, p].reshape(size, 2 * units)
            both += jnp.dot(x[:, at], piece, preferred_element_type=jnp.float32)
        gate = both[:, :units] * scale[0:1]
        up = both[:, units:] * scale[1:2]
        inner.append((gate / (1.0 + jnp.exp(-gate)) * up).astype(jnp.bfloat16))
    for p, at in enumerate(places):
        rows = slice(p * size, (p + 1) * size)
        total = dot_t(inner[0], down[rows]) + dot_t(inner[1], other_down[rows])
        out[:, at] = total.astype(jnp.bfloat16)


def mlp(labels, x, *weights):
    shape = jax.ShapeDtypeStruct(x.shape, jnp.bfloat16)
    size = sum(w.size for w in weights)
    call = local_call(mlp_kernel, shape, [SMEM] + [VMEM] * 7, 2 * x.shape[0] * size, 2 * size)
    return call(labels, x, *weights)


def per_device(
    tokens,
    mix_gain,
    w_query,
    w_key,
    w_value,
    w_out,
    scale_query,
    scale_key,
    scale_value,
    scale_out,
    decay_rate,
    mlp_gain,
    w_gate,
    w_up,
    w_down,
    scale_gate,
    scale_up,
    scale_down,
):
    bf16, f32 = jnp.bfloat16, jnp.float32
    own_rows = tokens[0]
    rows, width = own_rows.shape
    length = rows * lax.axis_size(TP)
    peers = lax.axis_size("y")
    heads = heads_shard(w_query, w_key, w_value, w_out, peers)
    heads = lax.all_to_all(heads, "y", 0, 0, tiled=True).reshape(-1, heads.shape[2])
    own, downs = mlp_shard(w_gate, w_up, w_down, peers)
    own = ring_blocks(own)
    weights = lax.all_gather(own, "y", axis=0)
    weights = hold(weights)
    others = swap_cores(weights)
    mlp_scales = jnp.stack([scale_gate, scale_up])
    other_scales = swap_cores(mlp_scales)
    heads = ring_halves(heads)
    downs = lax.all_to_all(downs, "y", 0, 0, tiled=True).reshape(-1, downs.shape[2])
    downs = ring_pieces(downs)
    downs = pack(downs)
    other_downs = swap_cores(downs)
    all_rows = lax.all_gather(own_rows, TP, axis=0, tiled=True)

    values = all_rows.astype(f32)
    normed = (values * inv_rms(values) * mix_gain).astype(bf16)
    product = ring_dot(normed, heads, 3 * HEAD_DIM)
    positions = jnp.arange(length, dtype=f32)
    inv_freq = 1.0 / ROPE_BASE ** (jnp.arange(0, HEAD_DIM, 2, dtype=f32) / HEAD_DIM)
    angles = positions[:, None] * inv_freq[None, :]
    scales = (scale_query, scale_key, scale_value)
    core = lax.axis_index("core").astype(jnp.int32)[None]
    kept, sent = retain(
        decay_rate, core, product, jnp.cos(angles), jnp.sin(angles), scales, heads
    )

    got = swap_cores(sent)
    chips = lax.axis_size("x")
    both = (kept + got.astype(f32)).astype(bf16).reshape(chips, rows, width)
    terms = lax.all_to_all(both, "x", 0, 0, tiled=True)
    slots = jnp.stack(ring_slots()).astype(jnp.int32)
    hidden, copies = settle(slots, terms, own_rows, scale_out, mlp_gain)
    mlp_in = lax.all_to_all(copies, "x", 0, 0, tiled=True).reshape(-1, width)
    labels = jnp.stack(ring_labels()).astype(jnp.int32)
    partial = mlp(
        labels, mlp_in, weights, others, downs, other_downs, mlp_scales, other_scales
    )
    terms = lax.all_to_all(partial.reshape(chips, rows, width), "x", 0, 0, tiled=True)
    channel = jnp.sum(terms.astype(f32), axis=0) * scale_down
    return (hidden.astype(f32) + channel).astype(bf16)[None]


def solution(mesh):
    grid = Mesh(mesh.devices.reshape(2, 4, 8, 4, 2), ("rep", "z", "y", "x", "core"))
    seqs, fs = ("rep", "z", "y"), ("z", "y")
    by_rows, by_cols = P(fs, TP), P(TP, fs)
    in_specs = (
        P(seqs, TP, None), P(), by_rows, by_rows, by_rows, by_cols,
        P(TP), P(TP), P(TP), P(), P(TP), P(),
        by_rows, by_rows, by_cols, P(TP), P(TP), P(),
    )

    return jax.shard_map(per_device, mesh=grid, in_specs=in_specs, out_specs=P(seqs, TP, None), check_vma=False)
```

```python
import jax
import jax.numpy as jnp
from jax import lax
from jax.experimental import pallas as pl
from jax.experimental.pallas import tpu as pltpu
from jax.sharding import Mesh, PartitionSpec as P


HEAD_DIM = 256
EPS = 1e-06
ROPE_BASE = 10000.0
RING = ("rep", "z")
TP = ("x", "core")


def inv_rms(values):
    return lax.rsqrt(jnp.mean(values * values, axis=-1, keepdims=True) + EPS)


def pairs(offset, n=8):
    out = []
    for a in range(offset, n + offset, 2):
        b = (a + 1) % n
        out += [(a % n, b), (b, a % n)]
    return out


def ring_pieces(block):
    half = block.shape[0] // 2
    even = lax.ppermute(block, RING, pairs(0))
    odd = lax.ppermute(block, RING, pairs(1))
    far_a = lax.ppermute(even[:half], RING, pairs(1))
    far_b = lax.ppermute(odd[half:], RING, pairs(0))
    return block, even, odd, far_a, far_b


def ring_labels():
    z = lax.axis_index("z")
    odd = z % 2
    return z, z + 1 - 2 * odd, (z + 3 + 2 * odd) % 4, (z + 2) % 4


def ring_slots():
    z, even, odd, _ = ring_labels()
    return [jnp.where(z == j, 0, jnp.where(even == j, 1, jnp.where(odd == j, 2, 3))) for j in range(4)]


def ring_blocks(block):
    half = block.shape[0] // 2
    even = lax.ppermute(block, RING, pairs(0))
    odd = lax.ppermute(block, RING, pairs(1))
    far_a = lax.ppermute(block[:half], RING, [(i, (i + 2) % 8) for i in range(8)])
    far_b = lax.ppermute(block[half:], RING, [(i, (i - 2) % 8) for i in range(8)])
    blocks = jnp.concatenate([block, even, odd, far_a, far_b], axis=0)
    return blocks.reshape(4, *block.shape)


def ring_dot(x, pieces, columns):
    size = pieces[0].shape[0]
    half = size // 2
    own_at, even_at, odd_at, far_at = ring_labels()
    starts = (own_at * size, even_at * size, odd_at * size, far_at * size, far_at * size + half)

    def term(start, piece):
        cut = lax.dynamic_slice_in_dim(x, start, piece.shape[0], 1)
        return jnp.dot(cut, piece[:, :columns], preferred_element_type=jnp.float32)

    return sum(term(start, piece) for start, piece in zip(starts, pieces))


def dot_t(a, b):
    return lax.dot_general(a, b, (((1,), (1,)), ((), ())), preferred_element_type=jnp.float32)


def sum_over_chips(partial):
    blocks = partial.reshape(lax.axis_size("x"), -1, partial.shape[1])
    return jnp.sum(lax.all_to_all(blocks, "x", 0, 0, tiled=True).astype(jnp.float32), axis=0)


def sum_on_chips(partial):
    half = partial.shape[0] // 2
    first, second = partial[:half], partial[half:]

    def swap(array, offset):
        return lax.ppermute(array, "x", pairs(offset, 4)).astype(jnp.float32)

    a = first.astype(jnp.float32) + swap(first, 0)
    b = second.astype(jnp.float32) + swap(second, 1)
    a, b = a.astype(jnp.bfloat16), b.astype(jnp.bfloat16)
    return jnp.concatenate(
        [a.astype(jnp.float32) + swap(a, 1), b.astype(jnp.float32) + swap(b, 0)],
        axis=0,
    )


def swap_cores(array):
    return lax.ppermute(array, "core", [(0, 1), (1, 0)])


def rotary(values, cosine, sine):
    half = values.shape[-1] // 2
    first = values[:, :half]
    second = values[:, half:]
    return jnp.concatenate(
        [first * cosine - second * sine, first * sine + second * cosine], axis=-1
    )


VMEM = pl.BlockSpec(memory_space=pltpu.VMEM)
SMEM = pl.BlockSpec(memory_space=pltpu.SMEM)


def local_call(kernel, out_shape, specs, flops, moved, out_specs=VMEM):
    return pl.pallas_call(
        kernel,
        out_shape=out_shape,
        in_specs=specs,
        out_specs=out_specs,
        compiler_params=pltpu.CompilerParams(vmem_limit_bytes=24 * 2**20),
        cost_estimate=pl.CostEstimate(flops=flops, bytes_accessed=moved, transcendentals=0),
    )


def heads_shard_kernel(query, keyed, valued, out_w, out, held, sems):
    width = query.shape[1]
    parts = (query, keyed, valued, out_w)
    copies = [pltpu.make_async_copy(w, held.at[i], sems.at[i]) for i, w in enumerate(parts)]
    for copy in copies:
        copy.start()
    for i, copy in enumerate(copies):
        copy.wait()
        part = held[i].astype(jnp.bfloat16)
        for peer in range(out.shape[0]):
            out[peer, :, i * width : (i + 1) * width] = part


def heads_shard(w_query, w_key, w_value, w_out, peers):
    rows, width = w_query.shape
    return pl.pallas_call(
        heads_shard_kernel,
        out_shape=jax.ShapeDtypeStruct((peers, rows, 4 * width), jnp.bfloat16),
        in_specs=[pl.BlockSpec(memory_space=pltpu.HBM)] * 4,
        out_specs=VMEM,
        scratch_shapes=[
            pltpu.VMEM((4, rows, width), jnp.float32),
            pltpu.SemaphoreType.DMA((4,)),
        ],
        compiler_params=pltpu.CompilerParams(vmem_limit_bytes=60 * 2**20),
        cost_estimate=pl.CostEstimate(flops=10**7, bytes_accessed=2**21, transcendentals=0),
        name="heads_shard",
    )(w_query, w_key, w_value, w_out.T)


def mlp_shard_kernel(gate, up, down, out):
    units = gate.shape[1]
    out[:, :units] = gate[...].astype(jnp.bfloat16)
    out[:, units : 2 * units] = up[...].astype(jnp.bfloat16)
    out[:, 2 * units :] = down[...].astype(jnp.bfloat16)


def mlp_shard(w_gate, w_up, w_down):
    rows, units = w_gate.shape
    shape = jax.ShapeDtypeStruct((rows, 3 * units), jnp.bfloat16)
    return local_call(mlp_shard_kernel, shape, [VMEM] * 3, 10**7, 2**20)(w_gate, w_up, w_down.T)


def retain_kernel(rate, core, product, cosine, sine, sq, sk, sv, own, even, odd, far_a, far_b, kept, sent):
    width = sq.shape[1]
    cos, sin = cosine[...], sine[...]
    query = rotary(product[:, :width] * sq[...], cos, sin).astype(jnp.bfloat16)
    keyed = rotary(product[:, width : 2 * width] * sk[...], cos, sin).astype(jnp.bfloat16)
    valued = (product[:, 2 * width :] * sv[...]).astype(jnp.bfloat16)
    length = product.shape[0]
    after = lax.broadcasted_iota(jnp.int32, (length, length), 0)
    before = lax.broadcasted_iota(jnp.int32, (length, length), 1)
    distance = (after - before).astype(jnp.float32)
    decay = jnp.exp(-rate[0] * jnp.maximum(distance, 0.0))
    weights = jnp.where(distance >= 0.0, dot_t(query, keyed) * decay, 0.0).astype(jnp.bfloat16)
    retained = jnp.dot(weights, valued, preferred_element_type=jnp.float32)
    attended = retained * inv_rms(retained)
    rows = length // 8
    first = [attended[i * rows : (i + 1) * rows] for i in range(0, 8, 2)]
    second = [attended[i * rows : (i + 1) * rows] for i in range(1, 8, 2)]
    low = core[0] == 0
    mine = [jnp.where(low, a, b) for a, b in zip(first, second)]
    other = [jnp.where(low, b, a) for a, b in zip(first, second)]
    attended = jnp.concatenate(mine + other, axis=0).astype(jnp.bfloat16)
    half = length // 2
    at = 0
    for piece in (own, even, odd, far_a, far_b):
        to = at + piece.shape[0]
        term = dot_t(attended, piece[:, 3 * width :])
        kept[:, at:to] = term[:half]
        sent[:, at:to] = term[half:].astype(jnp.bfloat16)
        at = to


def retain(rate, core, product, cosine, sine, scales, pieces):
    columns = sum(piece.shape[0] for piece in pieces)
    half = product.shape[0] // 2
    shapes = [jax.ShapeDtypeStruct((half, columns), kind) for kind in (jnp.float32, jnp.bfloat16)]
    specs = [SMEM] * 2 + [VMEM] * (6 + len(pieces))
    scales = [scale[None] for scale in scales]
    return local_call(retain_kernel, shapes, specs, 3 * 10**8, 2**21, [VMEM] * 2)(
        rate, core, product, cosine, sine, *scales, *pieces
    )


def mlp_kernel(labels, x, weights, others, scales, other_scales, out, held, sems):
    units = scales.shape[1]
    size = x.shape[1] // 4
    copies = [
        [pltpu.make_async_copy(w.at[:, p], held.at[i, p], sems.at[i, p]) for p in range(4)]
        for i, w in enumerate((weights, others))
    ]
    for copy in copies[0] + copies[1]:
        copy.start()
    places = [pl.ds(pl.multiple_of(labels[p] * size, size), size) for p in range(4)]
    inner = []
    for i, scale in enumerate((scales, other_scales)):
        both = jnp.zeros((x.shape[0], 2 * units), jnp.float32)
        for p, at in enumerate(places):
            copies[i][p].wait()
            piece = held[i, p, :, :, : 2 * units].reshape(size, 2 * units)
            both += jnp.dot(x[:, at], piece, preferred_element_type=jnp.float32)
        gate = both[:, :units] * scale[0:1]
        up = both[:, units:] * scale[1:2]
        inner.append((gate / (1.0 + jnp.exp(-gate)) * up).astype(jnp.bfloat16))
    for p, at in enumerate(places):
        total = 0.0
        for i, part in enumerate(inner):
            total += dot_t(part, held[i, p, :, :, 2 * units :].reshape(size, units))
        out[:, at] = total.astype(jnp.bfloat16)


def mlp(labels, x, weights, others, scales, other_scales):
    hbm = pl.BlockSpec(memory_space=pltpu.HBM)
    peers, pieces = weights.shape[:2]
    return pl.pallas_call(
        mlp_kernel,
        out_shape=jax.ShapeDtypeStruct(x.shape, jnp.bfloat16),
        in_specs=[SMEM, VMEM, hbm, hbm, VMEM, VMEM],
        out_specs=VMEM,
        scratch_shapes=[
            pltpu.VMEM((2, pieces, peers, *weights.shape[2:]), jnp.bfloat16),
            pltpu.SemaphoreType.DMA((2, pieces)),
        ],
        compiler_params=pltpu.CompilerParams(vmem_limit_bytes=57 * 2**20),
        cost_estimate=pl.CostEstimate(
            flops=4 * x.shape[0] * weights.size, bytes_accessed=4 * weights.size, transcendentals=0
        ),
        name="mlp",
    )(labels, x, weights, others, scales, other_scales)


def per_device(
    tokens,
    mix_gain,
    w_query,
    w_key,
    w_value,
    w_out,
    scale_query,
    scale_key,
    scale_value,
    scale_out,
    decay_rate,
    mlp_gain,
    w_gate,
    w_up,
    w_down,
    scale_gate,
    scale_up,
    scale_down,
):
    bf16, f32 = jnp.bfloat16, jnp.float32
    own_rows = tokens[0]
    rows, width = own_rows.shape
    length = rows * lax.axis_size(TP)
    peers = lax.axis_size("y")
    heads = heads_shard(w_query, w_key, w_value, w_out, peers)
    heads = lax.all_to_all(heads, "y", 0, 0, tiled=True).reshape(-1, heads.shape[2])
    own = ring_blocks(mlp_shard(w_gate, w_up, w_down))
    mlp_weights = lax.all_gather(own, "y", axis=0)
    mlp_others = swap_cores(mlp_weights)
    mlp_scales = jnp.stack([scale_gate, scale_up])
    other_scales = swap_cores(mlp_scales)
    heads = ring_pieces(heads)
    all_rows = lax.all_gather(own_rows, TP, axis=0, tiled=True)

    values = all_rows.astype(f32)
    normed = (values * inv_rms(values) * mix_gain).astype(bf16)
    product = ring_dot(normed, heads, 3 * HEAD_DIM)
    positions = jnp.arange(length, dtype=f32)
    inv_freq = 1.0 / ROPE_BASE ** (jnp.arange(0, HEAD_DIM, 2, dtype=f32) / HEAD_DIM)
    angles = positions[:, None] * inv_freq[None, :]
    scales = (scale_query, scale_key, scale_value)
    core = lax.axis_index("core").astype(jnp.int32)[None]
    kept, sent = retain(
        decay_rate, core, product, jnp.cos(angles), jnp.sin(angles), scales, heads
    )

    slots = ring_slots()

    def in_order(values):
        size = width // 4
        return jnp.concatenate(
            [lax.dynamic_slice_in_dim(values, slot * size, size, 1) for slot in slots], axis=1
        )

    got = swap_cores(sent)
    mixed = sum_on_chips((kept + got.astype(f32)).astype(bf16))
    mixed = in_order(mixed) * scale_out
    chips = lax.axis_size("x")
    core_rows = all_rows.reshape(chips, 2, rows, width)
    core_rows = lax.dynamic_index_in_dim(core_rows, lax.axis_index("core"), 1, keepdims=False)
    hidden = (core_rows.reshape(-1, width).astype(f32) + mixed).astype(bf16)
    values = hidden.astype(f32)
    mlp_in = (values * inv_rms(values) * mlp_gain).astype(bf16)
    hidden = lax.dynamic_slice_in_dim(hidden, lax.axis_index("x") * rows, rows, 0)
    labels = jnp.stack(ring_labels()).astype(jnp.int32)
    partial = mlp(labels, mlp_in, mlp_weights, mlp_others, mlp_scales, other_scales)
    channel = sum_over_chips(partial) * scale_down
    return (hidden.astype(f32) + channel).astype(bf16)[None]


def solution(mesh):
    grid = Mesh(mesh.devices.reshape(2, 4, 8, 4, 2), ("rep", "z", "y", "x", "core"))
    seqs, fs = ("rep", "z", "y"), ("z", "y")
    by_rows, by_cols = P(fs, TP), P(TP, fs)
    in_specs = (
        P(seqs, TP, None), P(), by_rows, by_rows, by_rows, by_cols,
        P(TP), P(TP), P(TP), P(), P(TP), P(),
        by_rows, by_rows, by_cols, P(TP), P(TP), P(),
    )

    return jax.shard_map(
        per_device, mesh=grid, in_specs=in_specs, out_specs=P(seqs, TP, None), check_vma=False
    )
```

```python
import jax
import jax.numpy as jnp
from jax import lax
from jax.experimental import pallas as pl
from jax.experimental.pallas import tpu as pltpu
from jax.sharding import Mesh, PartitionSpec as P


HEAD_DIM = 256
EPS = 1e-06
ROPE_BASE = 10000.0
RING = ("rep", "z")
TP = ("x", "core")


def inv_rms(values):
    return lax.rsqrt(jnp.mean(values * values, axis=-1, keepdims=True) + EPS)


def pairs(offset, n=8):
    out = []
    for a in range(offset, n + offset, 2):
        b = (a + 1) % n
        out += [(a % n, b), (b, a % n)]
    return out


def ring_pieces(block):
    half = block.shape[0] // 2
    even = lax.ppermute(block, RING, pairs(0))
    odd = lax.ppermute(block, RING, pairs(1))
    far_a = lax.ppermute(even[:half], RING, pairs(1))
    far_b = lax.ppermute(odd[half:], RING, pairs(0))
    return block, even, odd, far_a, far_b


def ring_labels():
    z = lax.axis_index("z")
    odd = z % 2
    return z, z + 1 - 2 * odd, (z + 3 + 2 * odd) % 4, (z + 2) % 4


def ring_slots():
    z, even, odd, _ = ring_labels()
    return [jnp.where(z == j, 0, jnp.where(even == j, 1, jnp.where(odd == j, 2, 3))) for j in range(4)]


def ring_dot(x, pieces, columns):
    size = pieces[0].shape[0]
    half = size // 2
    own_at, even_at, odd_at, far_at = ring_labels()
    starts = (own_at * size, even_at * size, odd_at * size, far_at * size, far_at * size + half)

    def term(start, piece):
        cut = lax.dynamic_slice_in_dim(x, start, piece.shape[0], 1)
        return jnp.dot(cut, piece[:, :columns], preferred_element_type=jnp.float32)

    total = sum(term(start, piece) for start, piece in zip(starts[:3], pieces[:3]))
    return total + term(starts[3], pieces[3]) + term(starts[4], pieces[4])


def dot_t(a, b):
    return lax.dot_general(a, b, (((1,), (1,)), ((), ())), preferred_element_type=jnp.float32)


def sum_over_chips(partial):
    blocks = partial.reshape(lax.axis_size("x"), -1, partial.shape[1])
    return jnp.sum(lax.all_to_all(blocks, "x", 0, 0, tiled=True).astype(jnp.float32), axis=0)


def swap_cores(array):
    return lax.ppermute(array, "core", [(0, 1), (1, 0)])


def rotary(values, cosine, sine):
    half = values.shape[-1] // 2
    first = values[:, :half]
    second = values[:, half:]
    return jnp.concatenate(
        [first * cosine - second * sine, first * sine + second * cosine], axis=-1
    )


VMEM = pl.BlockSpec(memory_space=pltpu.VMEM)
SMEM = pl.BlockSpec(memory_space=pltpu.SMEM)


def local_call(kernel, out_shape, specs, flops, moved, out_specs=VMEM):
    return pl.pallas_call(
        kernel,
        out_shape=out_shape,
        in_specs=specs,
        out_specs=out_specs,
        compiler_params=pltpu.CompilerParams(vmem_limit_bytes=24 * 2**20),
        cost_estimate=pl.CostEstimate(flops=flops, bytes_accessed=moved, transcendentals=0),
    )


def heads_shard_kernel(query, keyed, valued, out_w, out, held, sems):
    width = query.shape[1]
    parts = (query, keyed, valued, out_w)
    copies = [pltpu.make_async_copy(w, held.at[i], sems.at[i]) for i, w in enumerate(parts)]
    for copy in copies:
        copy.start()
    for i, copy in enumerate(copies):
        copy.wait()
        part = held[i].astype(jnp.bfloat16)
        for peer in range(out.shape[0]):
            out[peer, :, i * width : (i + 1) * width] = part


def heads_shard(w_query, w_key, w_value, w_out, peers):
    rows, width = w_query.shape
    return pl.pallas_call(
        heads_shard_kernel,
        out_shape=jax.ShapeDtypeStruct((peers, rows, 4 * width), jnp.bfloat16),
        in_specs=[pl.BlockSpec(memory_space=pltpu.HBM)] * 4,
        out_specs=VMEM,
        scratch_shapes=[
            pltpu.VMEM((4, rows, width), jnp.float32),
            pltpu.SemaphoreType.DMA((4,)),
        ],
        compiler_params=pltpu.CompilerParams(vmem_limit_bytes=60 * 2**20),
        cost_estimate=pl.CostEstimate(flops=10**7, bytes_accessed=2**21, transcendentals=0),
        name="heads_shard",
    )(w_query, w_key, w_value, w_out.T)


def mlp_shard_kernel(gate, up, down, out):
    units = gate.shape[1]
    for i, ref in enumerate((gate, up, down)):
        part = ref[...].astype(jnp.bfloat16)
        for peer in range(out.shape[0]):
            out[peer, :, i * units : (i + 1) * units] = part


def mlp_shard(w_gate, w_up, w_down, peers):
    rows, units = w_gate.shape
    shape = jax.ShapeDtypeStruct((peers, rows, 3 * units), jnp.bfloat16)
    return local_call(mlp_shard_kernel, shape, [VMEM] * 3, 10**7, 2**21)(w_gate, w_up, w_down.T)


def retain_kernel(rate, core, product, cosine, sine, sq, sk, sv, own, even, odd, far_a, far_b, kept, sent):
    width = sq.shape[1]
    cos, sin = cosine[...], sine[...]
    query = rotary(product[:, :width] * sq[...], cos, sin).astype(jnp.bfloat16)
    keyed = rotary(product[:, width : 2 * width] * sk[...], cos, sin).astype(jnp.bfloat16)
    valued = (product[:, 2 * width :] * sv[...]).astype(jnp.bfloat16)
    length = product.shape[0]
    after = lax.broadcasted_iota(jnp.int32, (length, length), 0)
    before = lax.broadcasted_iota(jnp.int32, (length, length), 1)
    distance = (after - before).astype(jnp.float32)
    decay = jnp.exp(-rate[0] * jnp.maximum(distance, 0.0))
    weights = jnp.where(distance >= 0.0, dot_t(query, keyed) * decay, 0.0).astype(jnp.bfloat16)
    retained = jnp.dot(weights, valued, preferred_element_type=jnp.float32)
    attended = retained * inv_rms(retained)
    rows = length // 8
    first = [attended[i * rows : (i + 1) * rows] for i in range(0, 8, 2)]
    second = [attended[i * rows : (i + 1) * rows] for i in range(1, 8, 2)]
    low = core[0] == 0
    mine = [jnp.where(low, a, b) for a, b in zip(first, second)]
    other = [jnp.where(low, b, a) for a, b in zip(first, second)]
    attended = jnp.concatenate(mine + other, axis=0).astype(jnp.bfloat16)
    half = length // 2
    at = 0
    for piece in (own, even, odd, far_a, far_b):
        to = at + piece.shape[0]
        term = dot_t(attended, piece[:, 3 * width :])
        kept[:, at:to] = term[:half]
        sent[:, at:to] = term[half:].astype(jnp.bfloat16)
        at = to


def retain(rate, core, product, cosine, sine, scales, pieces):
    columns = sum(piece.shape[0] for piece in pieces)
    half = product.shape[0] // 2
    shapes = [jax.ShapeDtypeStruct((half, columns), kind) for kind in (jnp.float32, jnp.bfloat16)]
    specs = [SMEM] * 2 + [VMEM] * (6 + len(pieces))
    scales = [scale[None] for scale in scales]
    return local_call(retain_kernel, shapes, specs, 3 * 10**8, 2**21, [VMEM] * 2)(
        rate, core, product, cosine, sine, *scales, *pieces
    )


def near_kernel(places, x, own, even, odd, out):
    size = own.shape[0]
    wide = out.shape[1]
    total = 0.0
    for i, piece in enumerate((own, even, odd)):
        at = pl.ds(pl.multiple_of(places[i] * size, size), size)
        total += jnp.dot(x[:, at], piece[:, :wide], preferred_element_type=jnp.float32)
    out[...] = total


def near(places, x, pieces, wide):
    shape = jax.ShapeDtypeStruct((x.shape[0], wide), jnp.float32)
    specs = [SMEM] + [VMEM] * 4
    return local_call(near_kernel, shape, specs, 4 * 10**8, 2**22)(places, x, *pieces)


def mlp_kernel(places, core, x, both, scales, own, even, odd, far_a, far_b, kept, sent, inner):
    units = scales.shape[1]
    size = own.shape[0]
    half = size // 2
    far = pl.multiple_of(places[3] * size, size)
    total = both[...]
    for i, piece in enumerate((far_a, far_b)):
        at = pl.ds(far + i * half, half)
        total += jnp.dot(x[:, at], piece[:, : 2 * units], preferred_element_type=jnp.float32)
    gate = total[:, :units] * scales[0:1]
    up = total[:, units:] * scales[1:2]
    inner[...] = (gate / (1.0 + jnp.exp(-gate)) * up).astype(jnp.bfloat16)
    rows = x.shape[0] // 2
    mine = inner[pl.ds(pl.multiple_of(core[0] * rows, rows), rows), :]
    other = inner[pl.ds(pl.multiple_of((1 - core[0]) * rows, rows), rows), :]
    attended = jnp.concatenate([mine, other], axis=0)
    starts = [pl.multiple_of(places[i] * size, size) for i in range(3)] + [far, far + half]
    for start, piece in zip(starts, (own, even, odd, far_a, far_b)):
        term = dot_t(attended, piece[:, 2 * units :])
        at = pl.ds(start, piece.shape[0])
        kept[:, at] = term[:rows]
        sent[:, at] = term[rows:].astype(jnp.bfloat16)


def mlp(places, core, x, both, scales, pieces):
    half = (x.shape[0] // 2, x.shape[1])
    return pl.pallas_call(
        mlp_kernel,
        out_shape=[jax.ShapeDtypeStruct(half, kind) for kind in (jnp.float32, jnp.bfloat16)],
        in_specs=[SMEM] * 2 + [VMEM] * 8,
        out_specs=[VMEM] * 2,
        scratch_shapes=[pltpu.VMEM((x.shape[0], scales.shape[1]), jnp.bfloat16)],
        compiler_params=pltpu.CompilerParams(vmem_limit_bytes=24 * 2**20),
        cost_estimate=pl.CostEstimate(flops=5 * 10**8, bytes_accessed=2**23, transcendentals=0),
        name="mlp",
    )(places, core, x, both, scales, *pieces)


def per_device(
    tokens,
    mix_gain,
    w_query,
    w_key,
    w_value,
    w_out,
    scale_query,
    scale_key,
    scale_value,
    scale_out,
    decay_rate,
    mlp_gain,
    w_gate,
    w_up,
    w_down,
    scale_gate,
    scale_up,
    scale_down,
):
    bf16, f32 = jnp.bfloat16, jnp.float32
    own_rows = tokens[0]
    rows, width = own_rows.shape
    length = rows * lax.axis_size(TP)
    peers = lax.axis_size("y")
    heads = heads_shard(w_query, w_key, w_value, w_out, peers)
    heads = lax.all_to_all(heads, "y", 0, 0, tiled=True).reshape(-1, heads.shape[2])
    weights = mlp_shard(w_gate, w_up, w_down, peers)
    weights = lax.all_to_all(weights, "y", 0, 0, tiled=True).reshape(-1, weights.shape[2])
    heads = ring_pieces(heads)
    weights = ring_pieces(weights)
    all_rows = lax.all_gather(own_rows, TP, axis=0, tiled=True)

    values = all_rows.astype(f32)
    normed = (values * inv_rms(values) * mix_gain).astype(bf16)
    product = ring_dot(normed, heads, 3 * HEAD_DIM)
    positions = jnp.arange(length, dtype=f32)
    inv_freq = 1.0 / ROPE_BASE ** (jnp.arange(0, HEAD_DIM, 2, dtype=f32) / HEAD_DIM)
    angles = positions[:, None] * inv_freq[None, :]
    scales = (scale_query, scale_key, scale_value)
    core = lax.axis_index("core").astype(jnp.int32)[None]
    kept, sent = retain(
        decay_rate, core, product, jnp.cos(angles), jnp.sin(angles), scales, heads
    )

    slots = ring_slots()

    def in_order(values):
        size = width // 4
        return jnp.concatenate(
            [lax.dynamic_slice_in_dim(values, slot * size, size, 1) for slot in slots], axis=1
        )

    got = swap_cores(sent)
    mixed = sum_over_chips((kept + got.astype(f32)).astype(bf16))
    mixed = in_order(mixed) * scale_out
    hidden = (own_rows.astype(f32) + mixed).astype(bf16)
    values = hidden.astype(f32)
    mlp_in = (values * inv_rms(values) * mlp_gain).astype(bf16)
    copies = jnp.broadcast_to(mlp_in[None], (lax.axis_size("x"), rows, width))
    mlp_in = lax.all_to_all(copies, "x", 0, 0, tiled=True).reshape(-1, width)
    mlp_in = lax.all_gather(mlp_in, "core", axis=0, tiled=True)

    places = jnp.stack(ring_labels()).astype(jnp.int32)
    scales = jnp.stack([scale_gate, scale_up])
    both = near(places, mlp_in, weights[:3], 2 * w_gate.shape[1])
    kept, sent = mlp(places, core, mlp_in, both, scales, weights)
    got = swap_cores(sent)
    channel = sum_over_chips((kept + got.astype(f32)).astype(bf16)) * scale_down
    return (hidden.astype(f32) + channel).astype(bf16)[None]


def solution(mesh):
    grid = Mesh(mesh.devices.reshape(2, 4, 8, 4, 2), ("rep", "z", "y", "x", "core"))
    seqs, fs = ("rep", "z", "y"), ("z", "y")
    by_rows, by_cols = P(fs, TP), P(TP, fs)
    in_specs = (
        P(seqs, TP, None), P(), by_rows, by_rows, by_rows, by_cols,
        P(TP), P(TP), P(TP), P(), P(TP), P(),
        by_rows, by_rows, by_cols, P(TP), P(TP), P(),
    )

    return jax.shard_map(
        per_device, mesh=grid, in_specs=in_specs, out_specs=P(seqs, TP, None), check_vma=False
    )
```

```python
import jax
import jax.numpy as jnp
from jax import lax
from jax.experimental import pallas as pl
from jax.experimental.pallas import tpu as pltpu
from jax.sharding import Mesh, PartitionSpec as P


HEAD_DIM = 256
EPS = 1e-06
ROPE_BASE = 10000.0
RING = ("rep", "z")
TP = ("x", "core")


def inv_rms(values):
    return lax.rsqrt(jnp.mean(values * values, axis=-1, keepdims=True) + EPS)


def pairs(offset, n=8):
    out = []
    for a in range(offset, n + offset, 2):
        b = (a + 1) % n
        out += [(a % n, b), (b, a % n)]
    return out


def ring_pieces(block):
    half = block.shape[0] // 2
    even = lax.ppermute(block, RING, pairs(0))
    odd = lax.ppermute(block, RING, pairs(1))
    far_a = lax.ppermute(even[:half], RING, pairs(1))
    far_b = lax.ppermute(odd[half:], RING, pairs(0))
    return block, even, odd, far_a, far_b


def ring_labels():
    z = lax.axis_index("z")
    odd = z % 2
    return z, z + 1 - 2 * odd, (z + 3 + 2 * odd) % 4, (z + 2) % 4


def ring_slots():
    z, even, odd, _ = ring_labels()
    return [jnp.where(z == j, 0, jnp.where(even == j, 1, jnp.where(odd == j, 2, 3))) for j in range(4)]


def ring_blocks(block):
    even = lax.ppermute(block, RING, pairs(0))
    odd = lax.ppermute(block, RING, pairs(1))
    far = lax.ppermute(block, RING, [(i, (i + 2) % 8) for i in range(8)])
    return jnp.stack([block, even, odd, far])


def ring_dot(x, pieces, columns):
    size = pieces[0].shape[0]
    half = size // 2
    own_at, even_at, odd_at, far_at = ring_labels()
    starts = (own_at * size, even_at * size, odd_at * size, far_at * size, far_at * size + half)

    def term(start, piece):
        cut = lax.dynamic_slice_in_dim(x, start, piece.shape[0], 1)
        return jnp.dot(cut, piece[:, :columns], preferred_element_type=jnp.float32)

    return sum(term(start, piece) for start, piece in zip(starts, pieces))


def dot_t(a, b):
    return lax.dot_general(a, b, (((1,), (1,)), ((), ())), preferred_element_type=jnp.float32)


def sum_over_chips(partial):
    blocks = partial.reshape(lax.axis_size("x"), -1, partial.shape[1])
    return jnp.sum(lax.all_to_all(blocks, "x", 0, 0, tiled=True).astype(jnp.float32), axis=0)


def swap_cores(array):
    return lax.ppermute(array, "core", [(0, 1), (1, 0)])


def rotary(values, cosine, sine):
    half = values.shape[-1] // 2
    first = values[:, :half]
    second = values[:, half:]
    return jnp.concatenate(
        [first * cosine - second * sine, first * sine + second * cosine], axis=-1
    )


VMEM = pl.BlockSpec(memory_space=pltpu.VMEM)
SMEM = pl.BlockSpec(memory_space=pltpu.SMEM)


def local_call(kernel, out_shape, specs, flops, moved, out_specs=VMEM, grant=24):
    return pl.pallas_call(
        kernel,
        out_shape=out_shape,
        in_specs=specs,
        out_specs=out_specs,
        compiler_params=pltpu.CompilerParams(vmem_limit_bytes=grant * 2**20),
        cost_estimate=pl.CostEstimate(flops=flops, bytes_accessed=moved, transcendentals=0),
    )


def heads_shard_kernel(query, keyed, valued, out_w, out, held, sems):
    width = query.shape[1]
    parts = (query, keyed, valued, out_w)
    copies = [pltpu.make_async_copy(w, held.at[i], sems.at[i]) for i, w in enumerate(parts)]
    for copy in copies:
        copy.start()
    for i, copy in enumerate(copies):
        copy.wait()
        part = held[i].astype(jnp.bfloat16)
        for peer in range(out.shape[0]):
            out[peer, :, i * width : (i + 1) * width] = part


def heads_shard(w_query, w_key, w_value, w_out, peers):
    rows, width = w_query.shape
    return pl.pallas_call(
        heads_shard_kernel,
        out_shape=jax.ShapeDtypeStruct((peers, rows, 4 * width), jnp.bfloat16),
        in_specs=[pl.BlockSpec(memory_space=pltpu.HBM)] * 4,
        out_specs=VMEM,
        scratch_shapes=[
            pltpu.VMEM((4, rows, width), jnp.float32),
            pltpu.SemaphoreType.DMA((4,)),
        ],
        compiler_params=pltpu.CompilerParams(vmem_limit_bytes=60 * 2**20),
        cost_estimate=pl.CostEstimate(flops=10**7, bytes_accessed=2**21, transcendentals=0),
        name="heads_shard",
    )(w_query, w_key, w_value, w_out.T)


def mlp_shard_kernel(gate, up, down, out):
    units = gate.shape[1]
    out[:, :units] = gate[...].astype(jnp.bfloat16)
    out[:, units : 2 * units] = up[...].astype(jnp.bfloat16)
    out[:, 2 * units :] = down[...].astype(jnp.bfloat16)


def mlp_shard(w_gate, w_up, w_down):
    rows, units = w_gate.shape
    shape = jax.ShapeDtypeStruct((rows, 3 * units), jnp.bfloat16)
    return local_call(mlp_shard_kernel, shape, [VMEM] * 3, 10**7, 2**20)(w_gate, w_up, w_down.T)


def retain_kernel(rate, core, product, cosine, sine, sq, sk, sv, own, even, odd, far_a, far_b, kept, sent):
    width = sq.shape[1]
    cos, sin = cosine[...], sine[...]
    query = rotary(product[:, :width] * sq[...], cos, sin).astype(jnp.bfloat16)
    keyed = rotary(product[:, width : 2 * width] * sk[...], cos, sin).astype(jnp.bfloat16)
    valued = (product[:, 2 * width :] * sv[...]).astype(jnp.bfloat16)
    length = product.shape[0]
    after = lax.broadcasted_iota(jnp.int32, (length, length), 0)
    before = lax.broadcasted_iota(jnp.int32, (length, length), 1)
    distance = (after - before).astype(jnp.float32)
    decay = jnp.exp(-rate[0] * jnp.maximum(distance, 0.0))
    weights = jnp.where(distance >= 0.0, dot_t(query, keyed) * decay, 0.0).astype(jnp.bfloat16)
    retained = jnp.dot(weights, valued, preferred_element_type=jnp.float32)
    attended = retained * inv_rms(retained)
    rows = length // 8
    first = [attended[i * rows : (i + 1) * rows] for i in range(0, 8, 2)]
    second = [attended[i * rows : (i + 1) * rows] for i in range(1, 8, 2)]
    low = core[0] == 0
    mine = [jnp.where(low, a, b) for a, b in zip(first, second)]
    other = [jnp.where(low, b, a) for a, b in zip(first, second)]
    attended = jnp.concatenate(mine + other, axis=0).astype(jnp.bfloat16)
    half = length // 2
    at = 0
    for piece in (own, even, odd, far_a, far_b):
        to = at + piece.shape[0]
        term = dot_t(attended, piece[:, 3 * width :])
        kept[:, at:to] = term[:half]
        sent[:, at:to] = term[half:].astype(jnp.bfloat16)
        at = to


def retain(rate, core, product, cosine, sine, scales, pieces):
    columns = sum(piece.shape[0] for piece in pieces)
    half = product.shape[0] // 2
    shapes = [jax.ShapeDtypeStruct((half, columns), kind) for kind in (jnp.float32, jnp.bfloat16)]
    specs = [SMEM] * 2 + [VMEM] * (6 + len(pieces))
    scales = [scale[None] for scale in scales]
    return local_call(retain_kernel, shapes, specs, 3 * 10**8, 2**21, [VMEM] * 2)(
        rate, core, product, cosine, sine, *scales, *pieces
    )


def mlp_kernel(labels, x, weights, others, scales, other_scales, out):
    units = scales.shape[1]
    size = x.shape[1] // 4
    places = [pl.ds(pl.multiple_of(labels[p] * size, size), size) for p in range(4)]
    inner = []
    for held, scale in ((weights, scales), (others, other_scales)):
        both = jnp.zeros((x.shape[0], 2 * units), jnp.float32)
        for p, at in enumerate(places):
            piece = held[:, p, :, : 2 * units].reshape(size, 2 * units)
            both += jnp.dot(x[:, at], piece, preferred_element_type=jnp.float32)
        gate = both[:, :units] * scale[0:1]
        up = both[:, units:] * scale[1:2]
        inner.append((gate / (1.0 + jnp.exp(-gate)) * up).astype(jnp.bfloat16))
    for p, at in enumerate(places):
        total = 0.0
        for held, part in zip((weights, others), inner):
            total += dot_t(part, held[:, p, :, 2 * units :].reshape(size, units))
        out[:, at] = total.astype(jnp.bfloat16)


def mlp(labels, x, weights, others, scales, other_scales):
    shape = jax.ShapeDtypeStruct(x.shape, jnp.bfloat16)
    flops = 4 * x.shape[0] * x.shape[1] * weights.shape[-1]
    moved = 4 * weights.size
    call = local_call(mlp_kernel, shape, [SMEM] + [VMEM] * 5, flops, moved, grant=57)
    return call(labels, x, weights, others, scales, other_scales)


def per_device(
    tokens,
    mix_gain,
    w_query,
    w_key,
    w_value,
    w_out,
    scale_query,
    scale_key,
    scale_value,
    scale_out,
    decay_rate,
    mlp_gain,
    w_gate,
    w_up,
    w_down,
    scale_gate,
    scale_up,
    scale_down,
):
    bf16, f32 = jnp.bfloat16, jnp.float32
    own_rows = tokens[0]
    rows, width = own_rows.shape
    length = rows * lax.axis_size(TP)
    peers = lax.axis_size("y")
    heads = heads_shard(w_query, w_key, w_value, w_out, peers)
    heads = lax.all_to_all(heads, "y", 0, 0, tiled=True).reshape(-1, heads.shape[2])
    own = ring_blocks(mlp_shard(w_gate, w_up, w_down))
    mlp_weights = lax.all_gather(own, "y", axis=0)
    mlp_others = swap_cores(mlp_weights)
    mlp_scales = jnp.stack([scale_gate, scale_up])
    other_scales = swap_cores(mlp_scales)
    heads = ring_pieces(heads)
    all_rows = lax.all_gather(own_rows, TP, axis=0, tiled=True)

    values = all_rows.astype(f32)
    normed = (values * inv_rms(values) * mix_gain).astype(bf16)
    product = ring_dot(normed, heads, 3 * HEAD_DIM)
    positions = jnp.arange(length, dtype=f32)
    inv_freq = 1.0 / ROPE_BASE ** (jnp.arange(0, HEAD_DIM, 2, dtype=f32) / HEAD_DIM)
    angles = positions[:, None] * inv_freq[None, :]
    scales = (scale_query, scale_key, scale_value)
    core = lax.axis_index("core").astype(jnp.int32)[None]
    kept, sent = retain(
        decay_rate, core, product, jnp.cos(angles), jnp.sin(angles), scales, heads
    )

    slots = ring_slots()

    def in_order(values):
        size = width // 4
        return jnp.concatenate(
            [lax.dynamic_slice_in_dim(values, slot * size, size, 1) for slot in slots], axis=1
        )

    got = swap_cores(sent)
    mixed = sum_over_chips((kept + got.astype(f32)).astype(bf16))
    mixed = in_order(mixed) * scale_out
    hidden = (own_rows.astype(f32) + mixed).astype(bf16)
    values = hidden.astype(f32)
    mlp_in = (values * inv_rms(values) * mlp_gain).astype(bf16)
    copies = jnp.broadcast_to(mlp_in[None], (lax.axis_size("x"), rows, width))
    mlp_in = lax.all_to_all(copies, "x", 0, 0, tiled=True).reshape(-1, width)

    labels = jnp.stack(ring_labels()).astype(jnp.int32)
    partial = mlp(labels, mlp_in, mlp_weights, mlp_others, mlp_scales, other_scales)
    channel = sum_over_chips(partial) * scale_down
    return (hidden.astype(f32) + channel).astype(bf16)[None]


def solution(mesh):
    grid = Mesh(mesh.devices.reshape(2, 4, 8, 4, 2), ("rep", "z", "y", "x", "core"))
    seqs, fs = ("rep", "z", "y"), ("z", "y")
    by_rows, by_cols = P(fs, TP), P(TP, fs)
    in_specs = (
        P(seqs, TP, None), P(), by_rows, by_rows, by_rows, by_cols,
        P(TP), P(TP), P(TP), P(), P(TP), P(),
        by_rows, by_rows, by_cols, P(TP), P(TP), P(),
    )

    return jax.shard_map(
        per_device, mesh=grid, in_specs=in_specs, out_specs=P(seqs, TP, None), check_vma=False
    )
```

```python
import jax
import jax.numpy as jnp
from jax import lax
from jax.experimental import pallas as pl
from jax.experimental.pallas import tpu as pltpu
from jax.sharding import Mesh, PartitionSpec as P


HEAD_DIM = 256
EPS = 1e-06
ROPE_BASE = 10000.0
RING = ("rep", "z")
TP = ("x", "core")


def inv_rms(values):
    return lax.rsqrt(jnp.mean(values * values, axis=-1, keepdims=True) + EPS)


def pairs(offset, n=8):
    out = []
    for a in range(offset, n + offset, 2):
        b = (a + 1) % n
        out += [(a % n, b), (b, a % n)]
    return out


def ring_halves(block):
    half = block.shape[0] // 2
    low, high = block[:half], block[half:]
    even1 = lax.ppermute(low, RING, pairs(0))
    odd2 = lax.ppermute(high, RING, pairs(1))
    even2 = lax.ppermute(high, RING, pairs(0))
    odd1 = lax.ppermute(low, RING, pairs(1))
    far_a = lax.ppermute(even1, RING, pairs(1))
    far_b = lax.ppermute(odd2, RING, pairs(0))
    return block, even1, even2, odd1, odd2, far_a, far_b


def ring_labels():
    z = lax.axis_index("z")
    odd = z % 2
    return z, z + 1 - 2 * odd, (z + 3 + 2 * odd) % 4, (z + 2) % 4


def ring_slots():
    z, even, odd, _ = ring_labels()
    return [jnp.where(z == j, 0, jnp.where(even == j, 1, jnp.where(odd == j, 2, 3))) for j in range(4)]


def ring_blocks(block):
    even = lax.ppermute(block, RING, pairs(0))
    odd = lax.ppermute(block, RING, pairs(1))
    far = lax.ppermute(block, RING, [(i, (i + 2) % 8) for i in range(8)])
    return jnp.stack([block, even, odd, far])


def ring_dot(x, pieces, columns):
    size = pieces[0].shape[0]
    half = size // 2
    own_at, even_at, odd_at, far_at = [label * size for label in ring_labels()]
    starts = (own_at, even_at, even_at + half, odd_at, odd_at + half, far_at, far_at + half)

    def term(start, piece):
        cut = lax.dynamic_slice_in_dim(x, start, piece.shape[0], 1)
        return jnp.dot(cut, piece[:, :columns], preferred_element_type=jnp.float32)

    return sum(term(start, piece) for start, piece in zip(starts, pieces))


def dot_t(a, b):
    return lax.dot_general(a, b, (((1,), (1,)), ((), ())), preferred_element_type=jnp.float32)


def sum_over_chips(partial):
    blocks = partial.reshape(lax.axis_size("x"), -1, partial.shape[1])
    return jnp.sum(lax.all_to_all(blocks, "x", 0, 0, tiled=True).astype(jnp.float32), axis=0)


def swap_cores(array):
    return lax.ppermute(array, "core", [(0, 1), (1, 0)])


def rotary(values, cosine, sine):
    half = values.shape[-1] // 2
    first = values[:, :half]
    second = values[:, half:]
    return jnp.concatenate(
        [first * cosine - second * sine, first * sine + second * cosine], axis=-1
    )


VMEM = pl.BlockSpec(memory_space=pltpu.VMEM)
SMEM = pl.BlockSpec(memory_space=pltpu.SMEM)


def local_call(kernel, out_shape, specs, flops, moved, out_specs=VMEM):
    return pl.pallas_call(
        kernel,
        out_shape=out_shape,
        in_specs=specs,
        out_specs=out_specs,
        compiler_params=pltpu.CompilerParams(vmem_limit_bytes=24 * 2**20),
        cost_estimate=pl.CostEstimate(flops=flops, bytes_accessed=moved, transcendentals=0),
    )


def heads_shard_kernel(query, keyed, valued, out_w, out, held, sems):
    width = query.shape[1]
    parts = (query, keyed, valued, out_w)
    copies = [pltpu.make_async_copy(w, held.at[i], sems.at[i]) for i, w in enumerate(parts)]
    for copy in copies:
        copy.start()
    for i, copy in enumerate(copies):
        copy.wait()
        part = held[i].astype(jnp.bfloat16)
        for peer in range(out.shape[0]):
            out[peer, :, i * width : (i + 1) * width] = part


def heads_shard(w_query, w_key, w_value, w_out, peers):
    rows, width = w_query.shape
    return pl.pallas_call(
        heads_shard_kernel,
        out_shape=jax.ShapeDtypeStruct((peers, rows, 4 * width), jnp.bfloat16),
        in_specs=[pl.BlockSpec(memory_space=pltpu.HBM)] * 4,
        out_specs=VMEM,
        scratch_shapes=[
            pltpu.VMEM((4, rows, width), jnp.float32),
            pltpu.SemaphoreType.DMA((4,)),
        ],
        compiler_params=pltpu.CompilerParams(vmem_limit_bytes=60 * 2**20),
        cost_estimate=pl.CostEstimate(flops=10**7, bytes_accessed=2**21, transcendentals=0),
        name="heads_shard",
    )(w_query, w_key, w_value, w_out.T)


def mlp_shard_kernel(gate, up, down, out):
    units = gate.shape[1]
    out[:, :units] = gate[...].astype(jnp.bfloat16)
    out[:, units : 2 * units] = up[...].astype(jnp.bfloat16)
    out[:, 2 * units :] = down[...].astype(jnp.bfloat16)


def mlp_shard(w_gate, w_up, w_down):
    rows, units = w_gate.shape
    shape = jax.ShapeDtypeStruct((rows, 3 * units), jnp.bfloat16)
    return local_call(mlp_shard_kernel, shape, [VMEM] * 3, 10**7, 2**20)(w_gate, w_up, w_down.T)


def retain_kernel(rate, core, product, cosine, sine, sq, sk, sv, *refs):
    pieces, (kept, sent) = refs[:-2], refs[-2:]
    width = sq.shape[1]
    cos, sin = cosine[...], sine[...]
    query = rotary(product[:, :width] * sq[...], cos, sin).astype(jnp.bfloat16)
    keyed = rotary(product[:, width : 2 * width] * sk[...], cos, sin).astype(jnp.bfloat16)
    valued = (product[:, 2 * width :] * sv[...]).astype(jnp.bfloat16)
    length = product.shape[0]
    after = lax.broadcasted_iota(jnp.int32, (length, length), 0)
    before = lax.broadcasted_iota(jnp.int32, (length, length), 1)
    distance = (after - before).astype(jnp.float32)
    decay = jnp.exp(-rate[0] * jnp.maximum(distance, 0.0))
    weights = jnp.where(distance >= 0.0, dot_t(query, keyed) * decay, 0.0).astype(jnp.bfloat16)
    retained = jnp.dot(weights, valued, preferred_element_type=jnp.float32)
    attended = retained * inv_rms(retained)
    rows = length // 8
    first = [attended[i * rows : (i + 1) * rows] for i in range(0, 8, 2)]
    second = [attended[i * rows : (i + 1) * rows] for i in range(1, 8, 2)]
    low = core[0] == 0
    mine = [jnp.where(low, a, b) for a, b in zip(first, second)]
    other = [jnp.where(low, b, a) for a, b in zip(first, second)]
    attended = jnp.concatenate(mine + other, axis=0).astype(jnp.bfloat16)
    half = length // 2
    at = 0
    for piece in pieces:
        to = at + piece.shape[0]
        term = dot_t(attended, piece[:, 3 * width :])
        kept[:, at:to] = term[:half]
        sent[:, at:to] = term[half:].astype(jnp.bfloat16)
        at = to


def retain(rate, core, product, cosine, sine, scales, pieces):
    columns = sum(piece.shape[0] for piece in pieces)
    half = product.shape[0] // 2
    shapes = [jax.ShapeDtypeStruct((half, columns), kind) for kind in (jnp.float32, jnp.bfloat16)]
    specs = [SMEM] * 2 + [VMEM] * (6 + len(pieces))
    scales = [scale[None] for scale in scales]
    return local_call(retain_kernel, shapes, specs, 3 * 10**8, 2**21, [VMEM] * 2)(
        rate, core, product, cosine, sine, *scales, *pieces
    )


def mlp_kernel(labels, x, weights, others, scales, other_scales, out):
    units = scales.shape[1]
    size = x.shape[1] // 4
    places = [pl.ds(pl.multiple_of(labels[p] * size, size), size) for p in range(4)]
    inner = []
    for held, scale in ((weights, scales), (others, other_scales)):
        both = jnp.zeros((x.shape[0], 2 * units), jnp.float32)
        for p, at in enumerate(places):
            piece = held[:, p, :, : 2 * units].reshape(size, 2 * units)
            both += jnp.dot(x[:, at], piece, preferred_element_type=jnp.float32)
        gate = both[:, :units] * scale[0:1]
        up = both[:, units:] * scale[1:2]
        inner.append((gate / (1.0 + jnp.exp(-gate)) * up).astype(jnp.bfloat16))
    for p, at in enumerate(places):
        total = 0.0
        for held, part in zip((weights, others), inner):
            total += dot_t(part, held[:, p, :, 2 * units :].reshape(size, units))
        out[:, at] = total.astype(jnp.bfloat16)


def mlp(labels, x, weights, others, scales, other_scales):
    shape = jax.ShapeDtypeStruct(x.shape, jnp.bfloat16)
    flops = 4 * x.shape[0] * x.shape[1] * weights.shape[-1]
    return local_call(mlp_kernel, shape, [SMEM] + [VMEM] * 5, flops, 4 * weights.size)(
        labels, x, weights, others, scales, other_scales
    )


def per_device(
    tokens,
    mix_gain,
    w_query,
    w_key,
    w_value,
    w_out,
    scale_query,
    scale_key,
    scale_value,
    scale_out,
    decay_rate,
    mlp_gain,
    w_gate,
    w_up,
    w_down,
    scale_gate,
    scale_up,
    scale_down,
):
    bf16, f32 = jnp.bfloat16, jnp.float32
    own_rows = tokens[0]
    rows, width = own_rows.shape
    length = rows * lax.axis_size(TP)
    peers = lax.axis_size("y")
    heads = heads_shard(w_query, w_key, w_value, w_out, peers)
    heads = lax.all_to_all(heads, "y", 0, 0, tiled=True).reshape(-1, heads.shape[2])
    own = ring_blocks(mlp_shard(w_gate, w_up, w_down))
    mlp_weights = lax.all_gather(own, "y", axis=0)
    mlp_others = swap_cores(mlp_weights)
    mlp_scales = jnp.stack([scale_gate, scale_up])
    other_scales = swap_cores(mlp_scales)
    heads = ring_halves(heads)
    all_rows = lax.all_gather(own_rows, TP, axis=0, tiled=True)

    values = all_rows.astype(f32)
    normed = (values * inv_rms(values) * mix_gain).astype(bf16)
    product = ring_dot(normed, heads, 3 * HEAD_DIM)
    positions = jnp.arange(length, dtype=f32)
    inv_freq = 1.0 / ROPE_BASE ** (jnp.arange(0, HEAD_DIM, 2, dtype=f32) / HEAD_DIM)
    angles = positions[:, None] * inv_freq[None, :]
    scales = (scale_query, scale_key, scale_value)
    core = lax.axis_index("core").astype(jnp.int32)[None]
    kept, sent = retain(
        decay_rate, core, product, jnp.cos(angles), jnp.sin(angles), scales, heads
    )

    slots = ring_slots()

    def in_order(values):
        size = width // 4
        return jnp.concatenate(
            [lax.dynamic_slice_in_dim(values, slot * size, size, 1) for slot in slots], axis=1
        )

    got = swap_cores(sent)
    mixed = sum_over_chips((kept + got.astype(f32)).astype(bf16))
    mixed = in_order(mixed) * scale_out
    hidden = (own_rows.astype(f32) + mixed).astype(bf16)
    values = hidden.astype(f32)
    mlp_in = (values * inv_rms(values) * mlp_gain).astype(bf16)
    copies = jnp.broadcast_to(mlp_in[None], (lax.axis_size("x"), rows, width))
    mlp_in = lax.all_to_all(copies, "x", 0, 0, tiled=True).reshape(-1, width)

    labels = jnp.stack(ring_labels()).astype(jnp.int32)
    partial = mlp(labels, mlp_in, mlp_weights, mlp_others, mlp_scales, other_scales)
    channel = sum_over_chips(partial) * scale_down
    return (hidden.astype(f32) + channel).astype(bf16)[None]


def solution(mesh):
    grid = Mesh(mesh.devices.reshape(2, 4, 8, 4, 2), ("rep", "z", "y", "x", "core"))
    seqs, fs = ("rep", "z", "y"), ("z", "y")
    by_rows, by_cols = P(fs, TP), P(TP, fs)
    in_specs = (
        P(seqs, TP, None), P(), by_rows, by_rows, by_rows, by_cols,
        P(TP), P(TP), P(TP), P(), P(TP), P(),
        by_rows, by_rows, by_cols, P(TP), P(TP), P(),
    )

    return jax.shard_map(
        per_device, mesh=grid, in_specs=in_specs, out_specs=P(seqs, TP, None), check_vma=False
    )
```

```python
import jax
import jax.numpy as jnp
from jax import lax
from jax.experimental import pallas as pl
from jax.experimental.pallas import tpu as pltpu
from jax.sharding import Mesh, PartitionSpec as P


HEAD_DIM = 256
EPS = 1e-06
ROPE_BASE = 10000.0
RING = ("rep", "z")
TP = ("x", "core")


def inv_rms(values):
    return lax.rsqrt(jnp.mean(values * values, axis=-1, keepdims=True) + EPS)


def pairs(offset, n=8):
    out = []
    for a in range(offset, n + offset, 2):
        b = (a + 1) % n
        out += [(a % n, b), (b, a % n)]
    return out


def ring_halves(block):
    half = block.shape[0] // 2
    low, high = block[:half], block[half:]
    even1 = lax.ppermute(low, RING, pairs(0))
    odd2 = lax.ppermute(high, RING, pairs(1))
    even2 = lax.ppermute(high, RING, pairs(0))
    odd1 = lax.ppermute(low, RING, pairs(1))
    far_a = lax.ppermute(even1, RING, pairs(1))
    far_b = lax.ppermute(odd2, RING, pairs(0))
    return block, even1, even2, odd1, odd2, far_a, far_b


def ring_labels():
    z = lax.axis_index("z")
    odd = z % 2
    return z, z + 1 - 2 * odd, (z + 3 + 2 * odd) % 4, (z + 2) % 4


def ring_slots():
    z, even, odd, _ = ring_labels()
    return [jnp.where(z == j, 0, jnp.where(even == j, 1, jnp.where(odd == j, 2, 3))) for j in range(4)]


def ring_blocks(block):
    even = lax.ppermute(block, RING, pairs(0))
    odd = lax.ppermute(block, RING, pairs(1))
    far = lax.ppermute(block, RING, [(i, (i + 2) % 8) for i in range(8)])
    return jnp.stack([block, even, odd, far])


def ring_dot(x, pieces, columns):
    size = pieces[0].shape[0]
    half = size // 2
    own_at, even_at, odd_at, far_at = [label * size for label in ring_labels()]
    starts = (own_at, even_at, even_at + half, odd_at, odd_at + half, far_at, far_at + half)

    def term(start, piece):
        cut = lax.dynamic_slice_in_dim(x, start, piece.shape[0], 1)
        return jnp.dot(cut, piece[:, :columns], preferred_element_type=jnp.float32)

    return sum(term(start, piece) for start, piece in zip(starts, pieces))


def dot_t(a, b):
    return lax.dot_general(a, b, (((1,), (1,)), ((), ())), preferred_element_type=jnp.float32)


def sum_over_chips(partial):
    blocks = partial.reshape(lax.axis_size("x"), -1, partial.shape[1])
    return jnp.sum(lax.all_to_all(blocks, "x", 0, 0, tiled=True).astype(jnp.float32), axis=0)


def swap_cores(array):
    return lax.ppermute(array, "core", [(0, 1), (1, 0)])


def rotary(values, cosine, sine):
    half = values.shape[-1] // 2
    first = values[:, :half]
    second = values[:, half:]
    return jnp.concatenate(
        [first * cosine - second * sine, first * sine + second * cosine], axis=-1
    )


VMEM = pl.BlockSpec(memory_space=pltpu.VMEM)
SMEM = pl.BlockSpec(memory_space=pltpu.SMEM)


def local_call(kernel, out_shape, specs, flops, moved, out_specs=VMEM):
    return pl.pallas_call(
        kernel,
        out_shape=out_shape,
        in_specs=specs,
        out_specs=out_specs,
        compiler_params=pltpu.CompilerParams(vmem_limit_bytes=24 * 2**20),
        cost_estimate=pl.CostEstimate(flops=flops, bytes_accessed=moved, transcendentals=0),
    )


def heads_shard_kernel(query, keyed, valued, out_w, out, held, sems):
    width = query.shape[1]
    parts = (query, keyed, valued, out_w)
    copies = [pltpu.make_async_copy(w, held.at[i], sems.at[i]) for i, w in enumerate(parts)]
    for copy in copies:
        copy.start()
    for i, copy in enumerate(copies):
        copy.wait()
        part = held[i].astype(jnp.bfloat16)
        for peer in range(out.shape[0]):
            out[peer, :, i * width : (i + 1) * width] = part


def heads_shard(w_query, w_key, w_value, w_out, peers):
    rows, width = w_query.shape
    return pl.pallas_call(
        heads_shard_kernel,
        out_shape=jax.ShapeDtypeStruct((peers, rows, 4 * width), jnp.bfloat16),
        in_specs=[pl.BlockSpec(memory_space=pltpu.HBM)] * 4,
        out_specs=VMEM,
        scratch_shapes=[
            pltpu.VMEM((4, rows, width), jnp.float32),
            pltpu.SemaphoreType.DMA((4,)),
        ],
        compiler_params=pltpu.CompilerParams(vmem_limit_bytes=60 * 2**20),
        cost_estimate=pl.CostEstimate(flops=10**7, bytes_accessed=2**21, transcendentals=0),
        name="heads_shard",
    )(w_query, w_key, w_value, w_out.T)


def mlp_shard_kernel(gate, up, down, out):
    units = gate.shape[1]
    out[:, :units] = gate[...].astype(jnp.bfloat16)
    out[:, units : 2 * units] = up[...].astype(jnp.bfloat16)
    out[:, 2 * units :] = down[...].astype(jnp.bfloat16)


def mlp_shard(w_gate, w_up, w_down):
    rows, units = w_gate.shape
    shape = jax.ShapeDtypeStruct((rows, 3 * units), jnp.bfloat16)
    return local_call(mlp_shard_kernel, shape, [VMEM] * 3, 10**7, 2**20)(w_gate, w_up, w_down.T)


def retain_kernel(rate, core, product, cosine, sine, sq, sk, sv, *refs):
    pieces, (kept, sent) = refs[:-2], refs[-2:]
    width = sq.shape[1]
    cos, sin = cosine[...], sine[...]
    query = rotary(product[:, :width] * sq[...], cos, sin).astype(jnp.bfloat16)
    keyed = rotary(product[:, width : 2 * width] * sk[...], cos, sin).astype(jnp.bfloat16)
    valued = (product[:, 2 * width :] * sv[...]).astype(jnp.bfloat16)
    length = product.shape[0]
    after = lax.broadcasted_iota(jnp.int32, (length, length), 0)
    before = lax.broadcasted_iota(jnp.int32, (length, length), 1)
    distance = (after - before).astype(jnp.float32)
    decay = jnp.exp(-rate[0] * jnp.maximum(distance, 0.0))
    weights = jnp.where(distance >= 0.0, dot_t(query, keyed) * decay, 0.0).astype(jnp.bfloat16)
    retained = jnp.dot(weights, valued, preferred_element_type=jnp.float32)
    attended = retained * inv_rms(retained)
    rows = length // 8
    first = [attended[i * rows : (i + 1) * rows] for i in range(0, 8, 2)]
    second = [attended[i * rows : (i + 1) * rows] for i in range(1, 8, 2)]
    low = core[0] == 0
    mine = [jnp.where(low, a, b) for a, b in zip(first, second)]
    other = [jnp.where(low, b, a) for a, b in zip(first, second)]
    attended = jnp.concatenate(mine + other, axis=0).astype(jnp.bfloat16)
    half = length // 2
    at = 0
    for piece in pieces:
        to = at + piece.shape[0]
        term = dot_t(attended, piece[:, 3 * width :])
        kept[:, at:to] = term[:half]
        sent[:, at:to] = term[half:].astype(jnp.bfloat16)
        at = to


def retain(rate, core, product, cosine, sine, scales, pieces):
    columns = sum(piece.shape[0] for piece in pieces)
    half = product.shape[0] // 2
    shapes = [jax.ShapeDtypeStruct((half, columns), kind) for kind in (jnp.float32, jnp.bfloat16)]
    specs = [SMEM] * 2 + [VMEM] * (6 + len(pieces))
    scales = [scale[None] for scale in scales]
    return local_call(retain_kernel, shapes, specs, 3 * 10**8, 2**21, [VMEM] * 2)(
        rate, core, product, cosine, sine, *scales, *pieces
    )


def hold_kernel(weights, out, sem):
    copy = pltpu.make_async_copy(weights.at[:, : out.shape[1]], out, sem)
    copy.start()
    copy.wait()


def hold(weights, count):
    shape = (weights.shape[0], count, *weights.shape[2:])
    return pl.pallas_call(
        hold_kernel,
        out_shape=jax.ShapeDtypeStruct(shape, weights.dtype),
        in_specs=[pl.BlockSpec(memory_space=pltpu.HBM)],
        out_specs=VMEM,
        scratch_shapes=[pltpu.SemaphoreType.DMA],
        compiler_params=pltpu.CompilerParams(vmem_limit_bytes=8 * 2**20),
        cost_estimate=pl.CostEstimate(flops=10**7, bytes_accessed=2**22, transcendentals=0),
        name="hold",
    )(weights)


def mlp_kernel(labels, x, early, late, others, scales, other_scales, out):
    units = scales.shape[1]
    size = x.shape[1] // 4
    places = [pl.ds(pl.multiple_of(labels[p] * size, size), size) for p in range(4)]
    first = early.shape[1]
    mine = [early[:, p] if p < first else late[:, p - first] for p in range(4)]
    theirs = [others[:, p] for p in range(4)]
    inner = []
    for held, scale in ((mine, scales), (theirs, other_scales)):
        both = jnp.zeros((x.shape[0], 2 * units), jnp.float32)
        for p, at in enumerate(places):
            piece = held[p][:, :, : 2 * units].reshape(size, 2 * units)
            both += jnp.dot(x[:, at], piece, preferred_element_type=jnp.float32)
        gate = both[:, :units] * scale[0:1]
        up = both[:, units:] * scale[1:2]
        inner.append((gate / (1.0 + jnp.exp(-gate)) * up).astype(jnp.bfloat16))
    for p, at in enumerate(places):
        total = 0.0
        for held, part in zip((mine, theirs), inner):
            total += dot_t(part, held[p][:, :, 2 * units :].reshape(size, units))
        out[:, at] = total.astype(jnp.bfloat16)


def mlp(labels, x, early, late, others, scales, other_scales):
    shape = jax.ShapeDtypeStruct(x.shape, jnp.bfloat16)
    flops = 4 * x.shape[0] * x.shape[1] * others.shape[-1]
    return local_call(mlp_kernel, shape, [SMEM] + [VMEM] * 6, flops, 4 * others.size)(
        labels, x, early, late, others, scales, other_scales
    )


def per_device(
    tokens,
    mix_gain,
    w_query,
    w_key,
    w_value,
    w_out,
    scale_query,
    scale_key,
    scale_value,
    scale_out,
    decay_rate,
    mlp_gain,
    w_gate,
    w_up,
    w_down,
    scale_gate,
    scale_up,
    scale_down,
):
    bf16, f32 = jnp.bfloat16, jnp.float32
    own_rows = tokens[0]
    rows, width = own_rows.shape
    length = rows * lax.axis_size(TP)
    peers = lax.axis_size("y")
    heads = heads_shard(w_query, w_key, w_value, w_out, peers)
    heads = lax.all_to_all(heads, "y", 0, 0, tiled=True).reshape(-1, heads.shape[2])
    own = ring_blocks(mlp_shard(w_gate, w_up, w_down))
    mlp_weights = lax.all_gather(own, "y", axis=0)
    mlp_others = swap_cores(mlp_weights)
    early = hold(mlp_weights, 2)
    mlp_scales = jnp.stack([scale_gate, scale_up])
    other_scales = swap_cores(mlp_scales)
    heads = ring_halves(heads)
    all_rows = lax.all_gather(own_rows, TP, axis=0, tiled=True)

    values = all_rows.astype(f32)
    normed = (values * inv_rms(values) * mix_gain).astype(bf16)
    product = ring_dot(normed, heads, 3 * HEAD_DIM)
    positions = jnp.arange(length, dtype=f32)
    inv_freq = 1.0 / ROPE_BASE ** (jnp.arange(0, HEAD_DIM, 2, dtype=f32) / HEAD_DIM)
    angles = positions[:, None] * inv_freq[None, :]
    scales = (scale_query, scale_key, scale_value)
    core = lax.axis_index("core").astype(jnp.int32)[None]
    kept, sent = retain(
        decay_rate, core, product, jnp.cos(angles), jnp.sin(angles), scales, heads
    )

    slots = ring_slots()

    def in_order(values):
        size = width // 4
        return jnp.concatenate(
            [lax.dynamic_slice_in_dim(values, slot * size, size, 1) for slot in slots], axis=1
        )

    got = swap_cores(sent)
    mixed = sum_over_chips((kept + got.astype(f32)).astype(bf16))
    mixed = in_order(mixed) * scale_out
    hidden = (own_rows.astype(f32) + mixed).astype(bf16)
    values = hidden.astype(f32)
    mlp_in = (values * inv_rms(values) * mlp_gain).astype(bf16)
    copies = jnp.broadcast_to(mlp_in[None], (lax.axis_size("x"), rows, width))
    mlp_in = lax.all_to_all(copies, "x", 0, 0, tiled=True).reshape(-1, width)

    labels = jnp.stack(ring_labels()).astype(jnp.int32)
    partial = mlp(labels, mlp_in, early, mlp_weights[:, 2:], mlp_others, mlp_scales, other_scales)
    channel = sum_over_chips(partial) * scale_down
    return (hidden.astype(f32) + channel).astype(bf16)[None]


def solution(mesh):
    grid = Mesh(mesh.devices.reshape(2, 4, 8, 4, 2), ("rep", "z", "y", "x", "core"))
    seqs, fs = ("rep", "z", "y"), ("z", "y")
    by_rows, by_cols = P(fs, TP), P(TP, fs)
    in_specs = (
        P(seqs, TP, None), P(), by_rows, by_rows, by_rows, by_cols,
        P(TP), P(TP), P(TP), P(), P(TP), P(),
        by_rows, by_rows, by_cols, P(TP), P(TP), P(),
    )

    return jax.shard_map(
        per_device, mesh=grid, in_specs=in_specs, out_specs=P(seqs, TP, None), check_vma=False
    )
```
